512 devices in a mesh: kv: 16 (over y, x), tp: 32 (over z, core).
Axes of the slice: x: 4, y: 4, z: 16, core: 2. Of those that a mesh axis runs over, the one named last changes fastest.
Arguments:
- tokens: bfloat16 [256, 4096], P('tp', 'kv'), may hold values from -100 to 100
- state: float32 [256, 32, 128, 128], P('kv', 'tp'), may hold values from -3 to 3
- gain_pre: bfloat16 [4096], P('kv'), may hold values from 0.099609375 to 1.8984375
- w_gate_pre: bfloat16 [4096, 11264], P('kv', 'tp'), may hold values from -0.09375 to 0.09375
- w_up_pre: bfloat16 [4096, 11264], P('kv', 'tp'), may hold values from -0.09375 to 0.09375
- w_down_pre: bfloat16 [11264, 4096], P('tp', 'kv'), may hold values from -0.109375 to 0.109375
- gain_mix: bfloat16 [4096], P('kv'), may hold values from 0.099609375 to 1.8984375
- w_query: bfloat16 [4096, 4096], P('kv', 'tp'), may hold values from -0.09375 to 0.09375
- w_key: bfloat16 [4096, 4096], P('kv', 'tp'), may hold values from -0.09375 to 0.09375
- w_value: bfloat16 [4096, 4096], P('kv', 'tp'), may hold values from -0.09375 to 0.09375
- w_decay: bfloat16 [4096, 32], P('kv'), may hold values from -0.09375 to 0.09375
- w_blend: bfloat16 [4096, 32], P('kv'), may hold values from -0.09375 to 0.09375
- decay_base: float32 [32], P('tp'), may hold values from -3 to 0.7
- decay_shift: float32 [32], P('tp'), may hold values from -2 to 0.5
- head_gain: bfloat16 [128], replicated, may hold values from 0.099609375 to 1.8984375
- w_out: bfloat16 [4096, 4096], P('tp', 'kv'), may hold values from -0.09375 to 0.09375
- gain_post: bfloat16 [4096], P('kv'), may hold values from 0.099609375 to 1.8984375
- w_gate_post: bfloat16 [4096, 11264], P('kv', 'tp'), may hold values from -0.09375 to 0.09375
- w_up_post: bfloat16 [4096, 11264], P('kv', 'tp'), may hold values from -0.09375 to 0.09375
- w_down_post: bfloat16 [11264, 4096], P('tp', 'kv'), may hold values from -0.109375 to 0.109375
Outputs:
- result: bfloat16 [256, 4096], P('tp', 'kv')
- new_state: float32 [256, 32, 128, 128], P('kv', 'tp')
The draws below stay inside these ranges and needn't reach their ends.
All inputs are finite; a program needn't handle non-finite values.
Results may differ from the reference program's by a relative error of at most 0.015.
Values may be sent and summed in bfloat16 or wider, within the bound.
No kernel may reach another device: no remote copies, remote signals or barrier semaphores. Data moves between devices by JAX's collectives and lax.ppermute only.
A program may use at most 64 MiB of HBM per device.

```python
import math
import jax
import jax.numpy as jnp
from jax import lax

D = 4096
FF = 11264
HEADS = 32
HEAD_DIM = 128
ROWS = 256
N_KV = 16
N_TP = 32


def draw_tokens(key, part):
    keys = jax.random.split(jax.random.fold_in(key, 11), 3)
    base = jnp.clip(jax.random.normal(keys[0], (ROWS, D), jnp.float32), -4.0, 4.0)
    rise_factor = 4.0
    low_end = 0.4
    high_end = 4.0
    row_scale = jnp.exp(jax.random.uniform(keys[1], (ROWS, 1), jnp.float32, math.log(low_end), math.log(high_end)))
    column_rise = jnp.exp(math.log(rise_factor) * jnp.arange(D, dtype=jnp.float32) / D)
    column_scale = column_rise * jax.random.uniform(keys[2], (D,), jnp.float32, 0.6, 1.4)
    return (base * row_scale * column_scale[None, :]).astype(jnp.bfloat16)


def block_levels(own_key, extent, cuts, smallest, high):
    loudness = 1.0
    for dim, shards_of in cuts:
        draws = jax.random.uniform(jax.random.fold_in(jax.random.fold_in(own_key, 6), dim), (shards_of,), jnp.float32, smallest / len(cuts), high / len(cuts))
        loudness = loudness * jnp.repeat(jnp.exp(draws), extent[dim] // shards_of).reshape((-1,) + (1,) * (len(extent) - 1 - dim))
    return loudness


def centred(stream_key, extent, width, limit, cuts=(), held_as=jnp.bfloat16):
    loudness = block_levels(stream_key, extent, cuts, -0.22, 0.18) if cuts else 1.0
    values = jax.random.normal(stream_key, extent, jnp.float32) * width * loudness
    return jnp.minimum(jnp.maximum(values, -limit), limit).astype(held_as)


def setup_inputs(seed: int = 0) -> dict:
    arg_keys = jax.random.split(jax.random.key(seed), 21)
    return {
        "tokens": draw_tokens(jax.random.fold_in(arg_keys[20], 71), 0),
        "state": centred(arg_keys[1], (ROWS, HEADS, HEAD_DIM, HEAD_DIM), 0.5, 3.0, ((0, 16), (1, 32)), jnp.float32),
        "gain_pre": jnp.clip(1.0 + 0.18 * jax.random.normal(arg_keys[2], (D,), jnp.float32), 0.099609375, 1.8984375).astype(jnp.bfloat16),
        "w_gate_pre": centred(arg_keys[3], (D, FF), D ** -0.5, 0.09375, ((0, 16), (1, 32))),
        "w_up_pre": centred(arg_keys[4], (D, FF), D ** -0.5, 0.09375, ((0, 16), (1, 32))),
        "w_down_pre": centred(arg_keys[5], (FF, D), (FF // 4) ** -0.5, 0.109375, ((0, 32), (1, 16))),
        "gain_mix": jnp.clip(1.0 + 0.18 * jax.random.normal(arg_keys[6], (D,), jnp.float32), 0.099609375, 1.8984375).astype(jnp.bfloat16),
        "w_query": centred(arg_keys[7], (D, HEADS * HEAD_DIM), D ** -0.5, 0.09375, ((0, 16), (1, 32))),
        "w_key": centred(arg_keys[8], (D, HEADS * HEAD_DIM), D ** -0.5, 0.09375, ((0, 16), (1, 32))),
        "w_value": centred(arg_keys[9], (D, HEADS * HEAD_DIM), D ** -0.5, 0.09375, ((0, 16), (1, 32))),
        "w_decay": centred(arg_keys[10], (D, HEADS), D ** -0.5, 0.09375, ((0, 16),)),
        "w_blend": centred(arg_keys[11], (D, HEADS), D ** -0.5, 0.09375, ((0, 16),)),
        "decay_base": jnp.clip(-3.0 + 3.7 * jax.random.uniform(arg_keys[12], (HEADS,), jnp.float32) ** block_levels(arg_keys[12], (HEADS,), ((0, 32),), -0.2, 0.2), -3.0, 0.7),
        "decay_shift": jnp.clip(-2.0 + 2.5 * jax.random.uniform(arg_keys[13], (HEADS,), jnp.float32) ** block_levels(arg_keys[13], (HEADS,), ((0, 32),), -0.2, 0.2), -2.0, 0.5),
        "head_gain": jnp.clip(1.0 + 0.18 * jax.random.normal(arg_keys[14], (HEAD_DIM,), jnp.float32), 0.099609375, 1.8984375).astype(jnp.bfloat16),
        "w_out": centred(arg_keys[15], (HEADS * HEAD_DIM, D), (HEADS * HEAD_DIM) ** -0.5, 0.09375, ((0, 32), (1, 16))),
        "gain_post": jnp.clip(1.0 + 0.18 * jax.random.normal(arg_keys[16], (D,), jnp.float32), 0.099609375, 1.8984375).astype(jnp.bfloat16),
        "w_gate_post": centred(arg_keys[17], (D, FF), D ** -0.5, 0.09375, ((0, 16), (1, 32))),
        "w_up_post": centred(arg_keys[18], (D, FF), D ** -0.5, 0.09375, ((0, 16), (1, 32))),
        "w_down_post": centred(arg_keys[19], (FF, D), (FF // 4) ** -0.5, 0.109375, ((0, 32), (1, 16))),
    }


EPS = 1e-06

def block_product(left, right, blocks):
    rows_all = left.shape[0]
    inner = left.shape[1] // blocks
    left_blocks = left.reshape(rows_all, blocks, inner).transpose(1, 0, 2)
    right_blocks = right.reshape(blocks, inner, right.shape[1])

    def add_block(running, pieces):
        product = jnp.dot(pieces[0], pieces[1], preferred_element_type=jnp.float32)
        rounded = lax.optimization_barrier(product.astype(jnp.bfloat16))
        return (running + rounded.astype(jnp.float32), None)
    start = jnp.zeros((rows_all, right.shape[1]), jnp.float32)
    running, unused = lax.scan(add_block, start, (left_blocks, right_blocks))
    return running

def inverse_rms(stream):
    values = stream.astype(jnp.float32)
    return lax.rsqrt(lax.optimization_barrier(jnp.mean(values * values, axis=1, keepdims=True)) + EPS)

def gained(stream, gain_vec):
    return (stream.astype(jnp.float32) * gain_vec.astype(jnp.float32)).astype(jnp.bfloat16)

def residual_add(stream, branch, weight):
    return (stream.astype(jnp.float32) + weight * branch).astype(jnp.bfloat16)

def unit_rows(values):
    return values * lax.rsqrt(lax.optimization_barrier(jnp.sum(values * values, axis=-1, keepdims=True)) + EPS)

def half_block(stream, gain_vec, w_gate, w_up, w_down):
    factor = inverse_rms(stream)
    scaled = gained(stream, gain_vec)
    gate_sum = factor * block_product(scaled, w_gate, N_KV)
    up_sum = factor * block_product(scaled, w_up, N_KV)
    hidden = (jax.nn.silu(gate_sum) * up_sum).astype(jnp.bfloat16)
    return block_product(hidden, w_down, N_TP)

def reference(tokens, state, gain_pre, w_gate_pre, w_up_pre, w_down_pre, gain_mix, w_query, w_key, w_value, w_decay, w_blend, decay_base, decay_shift, head_gain, w_out, gain_post, w_gate_post, w_up_post, w_down_post):
    first = residual_add(tokens, half_block(tokens, gain_pre, w_gate_pre, w_up_pre, w_down_pre), 0.5)
    factor = inverse_rms(first)
    scaled = gained(first, gain_mix)
    rows_all = first.shape[0]
    heads = state.shape[1]
    head_dim = state.shape[3]
    queries = (factor * block_product(scaled, w_query, N_KV)).reshape(rows_all, heads, head_dim)
    keys_new = (factor * block_product(scaled, w_key, N_KV)).reshape(rows_all, heads, head_dim)
    values_new = (factor * block_product(scaled, w_value, N_KV)).reshape(rows_all, heads, head_dim)
    decay_in = factor * block_product(scaled, w_decay, N_KV)
    blend_in = factor * block_product(scaled, w_blend, N_KV)
    queries = unit_rows(queries) * head_dim ** (-0.5)
    keys_unit = unit_rows(keys_new)
    log_rate = -jnp.exp(decay_base.astype(jnp.float32)) * jax.nn.softplus(decay_in + decay_shift.astype(jnp.float32))
    rate = jnp.exp(log_rate)
    beta = jax.nn.sigmoid(blend_in)
    recalled = jnp.einsum('bhk,bhkv->bhv', keys_unit, state, precision=lax.Precision.HIGHEST)
    correction = beta[:, :, None] * (values_new - rate[:, :, None] * recalled)
    new_state = rate[:, :, None, None] * state + keys_unit[:, :, :, None] * correction[:, :, None, :]
    read_out = jnp.einsum('bhk,bhkv->bhv', queries, new_state, precision=lax.Precision.HIGHEST)
    normed = read_out * lax.rsqrt(lax.optimization_barrier(jnp.mean(read_out * read_out, axis=2, keepdims=True)) + EPS)
    normed = (normed * head_gain.astype(jnp.float32)).astype(jnp.bfloat16).reshape(rows_all, heads * head_dim)
    second = residual_add(first, block_product(normed, w_out, N_TP), 1.0)
    result = residual_add(second, half_block(second, gain_post, w_gate_post, w_up_post, w_down_post), 0.5)
    return (result, new_state)
```

```python
import jax
import jax.numpy as jnp
from jax import lax
from jax.sharding import Mesh
from jax.sharding import PartitionSpec as P

D = 4096
KV = ("kv_0", "kv_1")


EPS = 1e-06


def copy_for_each(x, axis):
    length = lax.axis_size(axis)
    return lax.all_to_all(jnp.broadcast_to(x[None], (length, *x.shape)), axis, 0, 0, tiled=True)


def joined_along(parts, dim):
    lengths = list(parts.shape[1:])
    lengths[dim] *= parts.shape[0]
    return jnp.moveaxis(parts, 0, dim).reshape(lengths)


def gathered_copies(x, axis, dim):
    parts = copy_for_each(x, axis)
    return joined_along(parts, dim)


def cut_along(x, dim, length):
    before, after = (x.shape[:dim], x.shape[dim + 1 :])
    return jnp.moveaxis(x.reshape(*before, length, -1, *after), dim, 0)


def sent_and_summed(x, axis, dim):
    length = lax.axis_size(axis)
    parts = lax.all_to_all(cut_along(x, dim, length), axis, 0, 0, tiled=True)
    return jnp.sum(parts.astype(jnp.float32), axis=0)


def split_widths(joined, widths):
    return tuple(jnp.split(joined, [sum(widths[:k]) for k in range(1, len(widths))], axis=1))


def spread(own_rows):
    return gathered_copies(own_rows, "tp", 0)


def square_sums(stream):
    values = stream.astype(jnp.float32)
    rest = jnp.sum(values * values, axis=1, keepdims=True)
    pieces = []
    for _ in range(3):
        piece = lax.reduce_precision(rest, exponent_bits=8, mantissa_bits=7)
        pieces.append(piece.astype(jnp.bfloat16))
        rest = rest - piece
    return pieces


def inverse_rms(summed_pieces):
    squares = jnp.sum(summed_pieces, axis=1, keepdims=True)
    return lax.rsqrt(squares / D + EPS)


def gained(stream, gain_vec):
    return (stream.astype(jnp.float32) * gain_vec.astype(jnp.float32)).astype(jnp.bfloat16)


def residual_add(stream, branch, weight):
    return (stream.astype(jnp.float32) + weight * branch).astype(jnp.bfloat16)


def unit_rows(values):
    return values * lax.rsqrt(jnp.sum(values * values, axis=-1, keepdims=True) + EPS)


def half_block(stream, gain_vec, w_gate, w_up, w_down):
    scaled = gained(stream, gain_vec)
    gate_part = jnp.dot(scaled, w_gate, preferred_element_type=jnp.float32)
    up_part = jnp.dot(scaled, w_up, preferred_element_type=jnp.float32)
    gate_sum, up_sum, squares = split_widths(
        sent_and_summed(
            jnp.concatenate(
                [
                    gate_part.astype(jnp.bfloat16),
                    up_part.astype(jnp.bfloat16),
                    *square_sums(stream),
                ],
                axis=1,
            ),
            KV,
            0,
        ),
        (w_gate.shape[1], w_up.shape[1], 3),
    )
    own_factor = inverse_rms(squares)
    hidden = (jax.nn.silu(own_factor * gate_sum) * (own_factor * up_sum)).astype(jnp.bfloat16)
    return jnp.dot(gathered_copies(hidden, KV, 0), w_down, preferred_element_type=jnp.float32)


def settle(partial_value):
    return sent_and_summed(partial_value.astype(jnp.bfloat16), "tp", 0)


def advance(own_rows, partial_value, weight):
    own_rows = residual_add(own_rows, settle(partial_value), weight)
    return (spread(own_rows), own_rows)


def on_device(
    tokens,
    state,
    gain_pre,
    w_gate_pre,
    w_up_pre,
    w_down_pre,
    gain_mix,
    w_query,
    w_key,
    w_value,
    w_decay,
    w_blend,
    decay_base,
    decay_shift,
    head_gain,
    w_out,
    gain_post,
    w_gate_post,
    w_up_post,
    w_down_post,
):
    own_rows = tokens
    stream = spread(own_rows)
    partial_value = half_block(stream, gain_pre, w_gate_pre, w_up_pre, w_down_pre)
    stream, own_rows = advance(own_rows, partial_value, 0.5)
    scaled = gained(stream, gain_mix)
    weights = (w_query, w_key, w_value, w_decay, w_blend)
    queries, keys_new, values_new, decay_in, blend_in, squares = split_widths(
        sent_and_summed(
            jnp.concatenate(
                [
                    *(
                        jnp.dot(scaled, w, preferred_element_type=jnp.float32).astype(jnp.bfloat16)
                        for w in weights
                    ),
                    *square_sums(stream),
                ],
                axis=1,
            ),
            KV,
            0,
        ),
        (*(w.shape[1] for w in weights), 3),
    )
    own_factor = inverse_rms(squares)
    seqs = state.shape[0]
    heads_dev = state.shape[1]
    head_dim = state.shape[3]
    queries = unit_rows((own_factor * queries).reshape(seqs, heads_dev, head_dim)) * head_dim ** (
        -0.5
    )
    keys_unit = unit_rows((own_factor * keys_new).reshape(seqs, heads_dev, head_dim))
    values_new = (own_factor * values_new).reshape(seqs, heads_dev, head_dim)
    head_start = lax.axis_index("tp") * heads_dev
    decay_in = lax.dynamic_slice_in_dim(own_factor * decay_in, head_start, heads_dev, 1)
    blend_in = lax.dynamic_slice_in_dim(own_factor * blend_in, head_start, heads_dev, 1)
    log_rate = -jnp.exp(decay_base) * jax.nn.softplus(decay_in + decay_shift)
    rate = jnp.exp(log_rate)
    beta = jax.nn.sigmoid(blend_in)
    recalled = jnp.einsum("bhk,bhkv->bhv", keys_unit, state, precision=lax.Precision.HIGHEST)
    correction = beta[:, :, None] * (values_new - rate[:, :, None] * recalled)
    new_state = (
        rate[:, :, None, None] * state + keys_unit[:, :, :, None] * correction[:, :, None, :]
    )
    read_out = jnp.einsum("bhk,bhkv->bhv", queries, new_state, precision=lax.Precision.HIGHEST)
    normed = read_out * lax.rsqrt(jnp.mean(read_out * read_out, axis=2, keepdims=True) + EPS)
    normed = (
        (normed * head_gain.astype(jnp.float32))
        .astype(jnp.bfloat16)
        .reshape(seqs, heads_dev * head_dim)
    )
    partial_value = jnp.dot(
        gathered_copies(normed, KV, 0), w_out, preferred_element_type=jnp.float32
    )
    stream, own_rows = advance(own_rows, partial_value, 1.0)
    partial_value = half_block(stream, gain_post, w_gate_post, w_up_post, w_down_post)
    result = residual_add(own_rows, settle(partial_value), 0.5)
    return (result, new_state)


def solution(mesh):
    finer = Mesh(mesh.devices.reshape(4, 4, mesh.shape["tp"]), ("kv_0", "kv_1", "tp"))
    in_specs = (
        P("tp", KV),
        P(KV, "tp", None, None),
        P(KV),
        P(KV, "tp"),
        P(KV, "tp"),
        P("tp", KV),
        P(KV),
        P(KV, "tp"),
        P(KV, "tp"),
        P(KV, "tp"),
        P(KV, None),
        P(KV, None),
        P("tp"),
        P("tp"),
        P(),
        P("tp", KV),
        P(KV),
        P(KV, "tp"),
        P(KV, "tp"),
        P("tp", KV),
    )
    out_specs = (P("tp", KV), P(KV, "tp", None, None))
    return jax.shard_map(
        on_device, mesh=finer, in_specs=in_specs, out_specs=out_specs, check_vma=False
    )
```

```python
import jax
import jax.numpy as jnp
from jax import lax
from jax.sharding import Mesh
from jax.sharding import PartitionSpec as P

D = 4096
EPS = 1e-06
KV = ("kv_0", "kv_1")
TP = ("z", "core")
KVC = ("kv_0", "kv_1", "core")
ALL = ("kv_0", "kv_1", "z", "core")
BF16 = jnp.bfloat16
F32 = jnp.float32


def dot_nn(a, b):
    return jnp.dot(a, b, preferred_element_type=F32)


def dot_nt(a, b):
    return lax.dot_general(a, b, (((1,), (1,)), ((), ())), preferred_element_type=F32)


def exchanged(parts, axis):
    return lax.all_to_all(parts, axis, 0, 0, tiled=True)


def copies(x, axis):
    return exchanged(jnp.broadcast_to(x[None], (lax.axis_size(axis), *x.shape)), axis)


def summed(parts, axis):
    return jnp.sum(exchanged(parts, axis).astype(F32), axis=0)


def from_partner(x):
    return lax.ppermute(x, "core", [(0, 1), (1, 0)])


def turned(x):
    n = lax.axis_size("z")
    pairs = [
        ((k * n + z) * 2 + c, (z * n + k) * 2 + c)
        for k in range(n)
        for z in range(n)
        for c in range(2)
    ]
    return lax.ppermute(x, ALL, pairs)


def square_sums(stream):
    values = stream.astype(F32)
    rest = jnp.sum(values * values, axis=1, keepdims=True)
    pieces = []
    for _ in range(3):
        piece = lax.reduce_precision(rest, exponent_bits=8, mantissa_bits=7)
        pieces.append(piece.astype(BF16))
        rest = rest - piece
    return pieces


def inverse_rms(summed_pieces):
    squares = jnp.sum(summed_pieces, axis=1, keepdims=True)
    return lax.rsqrt(squares / D + EPS)


def gained(stream, gain_vec):
    return (stream.astype(F32) * gain_vec.astype(F32)).astype(BF16)


def residual_add(stream, branch, weight):
    return (stream.astype(F32) + weight * branch).astype(BF16)


def unit_rows(values):
    return values * lax.rsqrt(jnp.sum(values * values, axis=-1, keepdims=True) + EPS)


def gated(sums, half):
    factor = inverse_rms(sums[:, 2 * half :])
    gate, up = factor * sums[:, :half], factor * sums[:, half : 2 * half]
    return (jax.nn.silu(gate) * up).astype(BF16)


def on_device(
    tokens,
    state,
    gain_pre,
    w_gate_pre,
    w_up_pre,
    w_down_pre,
    gain_mix,
    w_query,
    w_key,
    w_value,
    w_decay,
    w_blend,
    decay_base,
    decay_shift,
    head_gain,
    w_out,
    gain_post,
    w_gate_post,
    w_up_post,
    w_down_post,
):
    n_kv = lax.axis_size(KV)
    rows, width = tokens.shape
    units = w_gate_pre.shape[1]
    head_dim = w_query.shape[1]
    core = lax.axis_index("core")

    later = jnp.concatenate([w_out, w_gate_post.T, w_up_post.T, w_down_post], axis=0)
    later = lax.all_gather(later, TP, axis=0, tiled=False)
    cuts = [0, head_dim, head_dim + units, head_dim + 2 * units, head_dim + 3 * units]
    w_out_all, w_gate_all, w_up_all, w_down_all = (
        later[:, a:b] for a, b in zip(cuts[:-1], cuts[1:], strict=True)
    )

    own = jnp.concatenate([w_gate_pre.T, w_up_pre.T, w_down_pre], axis=0)
    other = from_partner(own)
    stream = copies(tokens, "z").reshape(-1, width)
    scaled = gained(stream, gain_pre)
    gate_own, up_own = dot_nt(scaled, own[:units]), dot_nt(scaled, own[units : 2 * units])
    gate_other, up_other = (
        dot_nt(scaled, other[:units]),
        dot_nt(scaled, other[units : 2 * units]),
    )
    sent = jnp.concatenate(
        [*(p.astype(BF16) for p in (gate_own, gate_other, up_own, up_other)), *square_sums(stream)],
        axis=1,
    )
    hidden = gated(summed(sent.reshape(n_kv, rows, -1), KV), 2 * units)
    hidden = copies(hidden, KV).reshape(-1, 2 * units)
    w_down = jnp.concatenate([own[2 * units :], other[2 * units :]], axis=0)
    branch = summed(dot_nn(hidden, w_down).astype(BF16).reshape(n_kv, rows, width), "z")
    first = residual_add(tokens, branch, 0.5)

    own = jnp.concatenate([w_query, w_key, w_value], axis=1)
    other = from_partner(own)
    pair = 2 * lax.axis_index("z")
    gates = jnp.concatenate(
        [
            lax.dynamic_slice_in_dim(w_decay.T, pair, 2, 0),
            lax.dynamic_slice_in_dim(w_blend.T, pair, 2, 0),
        ],
        axis=0,
    )
    stream = copies(first, "z").reshape(-1, width)
    scaled = gained(stream, gain_mix)
    own_part, other_part = dot_nn(scaled, own).astype(BF16), dot_nn(scaled, other).astype(BF16)
    gate_part = dot_nt(scaled, gates).astype(BF16)
    pieces = square_sums(stream)
    sent = jnp.stack(
        [
            jnp.concatenate(
                [
                    jnp.where(core == to, own_part, other_part),
                    gate_part[:, to : to + 1],
                    gate_part[:, 2 + to : 3 + to],
                    *pieces,
                ],
                axis=1,
            ).reshape(n_kv, rows, -1)
            for to in range(2)
        ],
        axis=1,
    )
    got = exchanged(sent.reshape(2 * n_kv, rows, -1), KVC)
    got = jnp.sum(got.reshape(n_kv, 2 * rows, -1).astype(F32), axis=0)
    factor = inverse_rms(got[:, 3 * head_dim + 2 :])
    got = factor * got[:, : 3 * head_dim + 2]
    queries = unit_rows(got[:, :head_dim]) * head_dim**-0.5
    keys = unit_rows(got[:, head_dim : 2 * head_dim])
    values = got[:, 2 * head_dim : 3 * head_dim]
    decay_in = got[:, 3 * head_dim : 3 * head_dim + 1]
    blend_in = got[:, 3 * head_dim + 1 :]
    rate = jnp.exp(-jnp.exp(decay_base) * jax.nn.softplus(decay_in + decay_shift))
    beta = jax.nn.sigmoid(blend_in)
    held = state[:, 0]
    recalled = jnp.einsum("bk,bkv->bv", keys, held, precision=lax.Precision.HIGHEST)
    correction = beta * (values - rate * recalled)
    new_state = rate[:, :, None] * held + keys[:, :, None] * correction[:, None, :]
    read_out = jnp.einsum("bk,bkv->bv", queries, new_state, precision=lax.Precision.HIGHEST)
    normed = read_out * lax.rsqrt(jnp.mean(read_out * read_out, axis=1, keepdims=True) + EPS)
    normed = (normed * head_gain.astype(F32)).astype(BF16)
    normed = turned(normed).reshape(1, 2, rows, head_dim)
    normed = exchanged(
        jnp.broadcast_to(normed, (n_kv, 2, rows, head_dim)).reshape(2 * n_kv, rows, head_dim), KVC
    )
    branch = jnp.einsum("trk,tkn->rn", normed, w_out_all, preferred_element_type=F32)
    second = residual_add(first, branch, 1.0)

    scaled = gained(second, gain_post)
    gate_part = jnp.einsum("rk,tnk->rtn", scaled, w_gate_all, preferred_element_type=F32)
    up_part = jnp.einsum("rk,tnk->rtn", scaled, w_up_all, preferred_element_type=F32)
    sent = jnp.concatenate(
        [
            gate_part.astype(BF16).reshape(rows, n_kv, 2 * units),
            up_part.astype(BF16).reshape(rows, n_kv, 2 * units),
            jnp.broadcast_to(
                jnp.concatenate(square_sums(second), axis=1)[:, None], (rows, n_kv, 3)
            ),
        ],
        axis=2,
    )
    hidden = gated(summed(jnp.moveaxis(sent, 1, 0), KV), 2 * units)
    hidden = copies(hidden, KV).reshape(n_kv, rows, 2, units)
    branch = jnp.einsum(
        "krcu,kcun->rn",
        hidden,
        w_down_all.reshape(n_kv, 2, units, width),
        preferred_element_type=F32,
    )
    result = residual_add(second, branch, 0.5)
    return (result, new_state[:, None])


def solution(mesh):
    finer = Mesh(mesh.devices.reshape(4, 4, mesh.shape["tp"] // 2, 2), ALL)
    in_specs = (
        P(TP, KV),
        P(KV, TP, None, None),
        P(KV),
        P(KV, TP),
        P(KV, TP),
        P(TP, KV),
        P(KV),
        P(KV, TP),
        P(KV, TP),
        P(KV, TP),
        P(KV, None),
        P(KV, None),
        P(TP),
        P(TP),
        P(),
        P(TP, KV),
        P(KV),
        P(KV, TP),
        P(KV, TP),
        P(TP, KV),
    )
    out_specs = (P(TP, KV), P(KV, TP, None, None))
    return jax.shard_map(
        on_device, mesh=finer, in_specs=in_specs, out_specs=out_specs, check_vma=False
    )
```

```python
import functools

import jax
import jax.numpy as jnp
from jax import lax
from jax.experimental import pallas as pl
from jax.experimental.pallas import tpu as pltpu
from jax.sharding import Mesh
from jax.sharding import PartitionSpec as P

D = 4096
EPS = 1e-06
KV = ("kv_0", "kv_1")
TP = ("z", "core")
KVC = ("kv_0", "kv_1", "core")
ALL = ("kv_0", "kv_1", "z", "core")
BF16 = jnp.bfloat16
F32 = jnp.float32


PAD = 384


def dot_nn(a, b):
    return jnp.dot(a, b, preferred_element_type=F32)


def dot_nt(a, b):
    return lax.dot_general(a, b, (((1,), (1,)), ((), ())), preferred_element_type=F32)


def exchanged(parts, axis):
    return lax.all_to_all(parts, axis, 0, 0, tiled=True)


def from_partner(x):
    return lax.ppermute(x, "core", [(0, 1), (1, 0)])


def local_call(kernel, shapes, args, *, scalars=0, far=(), scratch=(), limit=None):
    specs = [
        pl.BlockSpec(
            memory_space=pltpu.SMEM if i < scalars else pl.ANY if i in far else pltpu.VMEM
        )
        for i in range(len(args))
    ]
    outs = tuple(jax.ShapeDtypeStruct(shape, dtype) for shape, dtype in shapes)
    return pl.pallas_call(
        kernel,
        out_shape=outs,
        in_specs=specs,
        out_specs=tuple(pl.BlockSpec(memory_space=pltpu.VMEM) for _ in outs),
        scratch_shapes=list(scratch),
        compiler_params=pltpu.CompilerParams(vmem_limit_bytes=limit),
    )(*args)


def rows_of(ref):
    values = ref[...].astype(F32)
    return values.reshape(values.shape[0] * values.shape[1], values.shape[2])


def in_three(total):
    high = total.astype(BF16)
    rest = total - high.astype(F32)
    middle = rest.astype(BF16)
    return (high, middle, (rest - middle.astype(F32)).astype(BF16))


def scale_of(squares):
    return lax.rsqrt(squares / D + EPS)


def gate_up_kernel(rows_ref, gain_ref, gate_ref, up_ref, other_ref, out_ref):
    units = gate_ref.shape[0]
    n, rows, _ = rows_ref.shape
    stream = rows_of(rows_ref)
    scaled = (stream * gain_ref[...].astype(F32)).astype(BF16)
    weights = (gate_ref[...], other_ref[:units], up_ref[...], other_ref[units : 2 * units])
    for i, weight in enumerate(weights):
        out_ref[:, :, i * PAD + units : (i + 1) * PAD] = jnp.zeros((n, rows, PAD - units), BF16)
        product = dot_nt(scaled, weight).reshape(n, rows, units)
        out_ref[:, :, i * PAD : i * PAD + units] = product.astype(BF16)
    pieces = in_three(jnp.sum(stream * stream, axis=1, keepdims=True))
    for i, piece in enumerate(pieces):
        out_ref[:, :, units + i : units + i + 1] = (
            piece.astype(F32).reshape(n, rows, 1).astype(BF16)
        )


def hidden_kernel(units, parts_ref, out_ref):
    total = jnp.sum(parts_ref[...].astype(F32), axis=0)
    squares = jnp.sum(total[:, units : units + 3], axis=1, keepdims=True)
    factor = scale_of(squares)
    gate, up = factor * total[:, : 2 * PAD], factor * total[:, 2 * PAD :]
    hidden = (gate * jax.nn.sigmoid(gate) * up).astype(BF16)
    for i in range(out_ref.shape[0]):
        out_ref[i] = hidden


def down_kernel(hidden_ref, own_ref, other_ref, out_ref):
    units = own_ref.shape[0]
    hidden = rows_of(hidden_ref).astype(BF16)
    total = dot_nn(hidden[:, :units], own_ref[...])
    total += dot_nn(hidden[:, PAD : PAD + units], other_ref[2 * units : 3 * units])
    out_ref[...] = total.reshape(out_ref.shape).astype(BF16)


def first_kernel(parts_ref, own_ref, first_ref, out_ref):
    branch = jnp.sum(parts_ref[...].astype(F32), axis=0)
    first = (own_ref[...].astype(F32) + 0.5 * branch).astype(BF16)
    first_ref[...] = first
    for i in range(out_ref.shape[0]):
        out_ref[i] = first


def query_kernel(core_ref, rows_ref, gain_ref, q_ref, k_ref, v_ref, other_ref, gates_ref, out_ref):
    n, rows, _ = rows_ref.shape
    dim = q_ref.shape[1]
    stream = rows_of(rows_ref)
    scaled = (stream * gain_ref[...].astype(F32)).astype(BF16)
    is_first = core_ref[0] == 0
    for i, weight in enumerate((q_ref, k_ref, v_ref)):
        own = dot_nn(scaled, weight[...])
        other = dot_nn(scaled, other_ref[:, i * dim : (i + 1) * dim])
        for to, part in enumerate(
            (jnp.where(is_first, own, other), jnp.where(is_first, other, own))
        ):
            out_ref[:, to, :, i * dim : (i + 1) * dim] = part.reshape(n, rows, dim).astype(BF16)
    gates = dot_nt(scaled, gates_ref[...])
    pieces = in_three(jnp.sum(stream * stream, axis=1, keepdims=True))
    for to in range(2):
        columns = [gates[:, to : to + 1], gates[:, 2 + to : 3 + to]]
        columns += [piece.astype(F32) for piece in pieces]
        for i, column in enumerate(columns):
            at = 3 * dim + i
            out_ref[:, to, :, at : at + 1] = column.reshape(n, rows, 1).astype(BF16)


def state_kernel(
    parts_ref, state_ref, base_ref, shift_ref, head_gain_ref, state_out_ref, out_ref, held
):
    dim = state_ref.shape[2]
    got = jnp.sum(parts_ref[...].astype(F32), axis=0)
    squares = jnp.sum(got[:, 3 * dim + 2 : 3 * dim + 5], axis=1, keepdims=True)
    got = scale_of(squares) * got[:, : 3 * dim + 2]
    queries, keys, values = (got[:, i * dim : (i + 1) * dim] for i in range(3))
    decay_in, blend_in = got[:, 3 * dim : 3 * dim + 1], got[:, 3 * dim + 1 : 3 * dim + 2]

    def unit(v):
        return v * lax.rsqrt(jnp.sum(v * v, axis=1, keepdims=True) + EPS)

    queries, keys = unit(queries) * dim**-0.5, unit(keys)
    inner = decay_in + shift_ref[...]
    soft = jnp.maximum(inner, 0.0) + jnp.log1p(jnp.exp(-jnp.abs(inner)))
    rate = jnp.exp(-jnp.exp(base_ref[...]) * soft)
    beta = jax.nn.sigmoid(blend_in)
    queries_t, keys_t = queries.T, keys.T
    for b in range(state_ref.shape[0]):
        old = state_ref[b]
        key, query = keys_t[:, b : b + 1], queries_t[:, b : b + 1]
        rate_b = rate[b : b + 1]
        recalled = jnp.sum(key * old, axis=0, keepdims=True)
        correction = beta[b : b + 1] * (values[b : b + 1] - rate_b * recalled)
        new = rate_b * old + key * correction
        state_out_ref[b] = new
        held[b : b + 1] = jnp.sum(query * new, axis=0, keepdims=True)
    read = held[...]
    normed = read * lax.rsqrt(jnp.mean(read * read, axis=1, keepdims=True) + EPS)
    normed = (normed * head_gain_ref[...].astype(F32)).astype(BF16)
    for i in range(out_ref.shape[0]):
        out_ref[i] = normed


def out_kernel(core_ref, heads_ref, own_ref, other_ref, out_ref):
    n, both, dim = heads_ref.shape
    heads = heads_ref[...].astype(F32)
    zero = heads[:, : both // 2].reshape(n * both // 2, dim).astype(BF16)
    one = heads[:, both // 2 :].reshape(n * both // 2, dim).astype(BF16)
    from_zero, from_one = dot_nn, dot_nn
    is_first = core_ref[0] == 0
    own, other = own_ref[...], other_ref[other_ref.shape[0] - dim :]
    total = from_zero(zero, jnp.where(is_first, own, other))
    total += from_one(one, jnp.where(is_first, other, own))
    out_ref[...] = total.reshape(out_ref.shape).astype(BF16)


def wide_kernel(
    units, parts_ref, first_ref, gain_ref, weights_ref, out_ref, second_ref, held, sems
):
    n, rows, _ = out_ref.shape

    def copy(k):
        return pltpu.make_async_copy(
            weights_ref.at[pl.ds(2 * k, 2), pl.ds(0, 2 * units)], held.at[k], sems.at[k]
        )

    for k in range(n):
        copy(k).start()
    branch = jnp.sum(parts_ref[...].astype(F32), axis=0)
    second = (first_ref[...].astype(F32) + branch).astype(BF16)
    second_ref[...] = second
    stream = second.astype(F32)
    scaled = (stream * gain_ref[...].astype(F32)).astype(BF16)
    pieces = in_three(jnp.sum(stream * stream, axis=1, keepdims=True))
    for k in range(n):
        copy(k).wait()
        for i in range(4):
            out_ref[k, :, i * PAD + units : (i + 1) * PAD] = jnp.zeros((rows, PAD - units), BF16)
            weight = held[k, i % 2, (i // 2) * units : (i // 2 + 1) * units]
            out_ref[k, :, i * PAD : i * PAD + units] = dot_nt(scaled, weight).astype(BF16)
        for i, piece in enumerate(pieces):
            out_ref[k, :, units + i : units + i + 1] = piece


def last_kernel(units, hidden_ref, second_ref, weights_ref, out_ref, held, sems):
    n = hidden_ref.shape[0]

    def copy(k):
        return pltpu.make_async_copy(
            weights_ref.at[pl.ds(2 * k, 2), pl.ds(2 * units, units)], held.at[k], sems.at[k]
        )

    for k in range(n):
        copy(k).start()
    total = jnp.zeros(out_ref.shape, F32)
    for k in range(n):
        copy(k).wait()
        for i in range(2):
            total += dot_nn(hidden_ref[k, :, i * PAD : i * PAD + units], held[k, i])
    out_ref[...] = (second_ref[...].astype(F32) + 0.5 * total).astype(BF16)


def on_device(
    tokens,
    state,
    gain_pre,
    w_gate_pre,
    w_up_pre,
    w_down_pre,
    gain_mix,
    w_query,
    w_key,
    w_value,
    w_decay,
    w_blend,
    decay_base,
    decay_shift,
    head_gain,
    w_out,
    gain_post,
    w_gate_post,
    w_up_post,
    w_down_post,
):
    n = lax.axis_size(KV)
    rows, width = tokens.shape
    units = w_gate_pre.shape[1]
    seqs, _, dim, _ = state.shape
    core = lax.axis_index("core").reshape(1)
    block = (n, rows, width)
    wide = (n, rows, 4 * PAD)
    narrow = (n, rows, 2 * PAD)

    later = jnp.concatenate([w_gate_post.T, w_up_post.T, w_down_post], axis=0)
    later = lax.all_gather(later, TP, axis=0, tiled=False)

    gate_t, up_t = w_gate_pre.T, w_up_pre.T
    other = from_partner(jnp.concatenate([gate_t, up_t, w_down_pre, w_out], axis=0))
    stream = exchanged(jnp.broadcast_to(tokens[None], block), "z")
    (sent,) = local_call(
        gate_up_kernel, [(wide, BF16)], (stream, gain_pre[None], gate_t, up_t, other)
    )
    (hidden,) = local_call(
        functools.partial(hidden_kernel, units), [(narrow, BF16)], (exchanged(sent, KV),)
    )
    (sent,) = local_call(
        down_kernel, [(block, BF16)], (exchanged(hidden, KV), w_down_pre, other)
    )
    first, sent = local_call(
        first_kernel, [(tokens.shape, BF16), (block, BF16)], (exchanged(sent, "z"), tokens)
    )

    other_query = from_partner(jnp.concatenate([w_query, w_key, w_value], axis=1))
    pair = 2 * lax.axis_index("z")
    gates = jnp.concatenate(
        [
            lax.dynamic_slice_in_dim(w_decay.T, pair, 2, 0),
            lax.dynamic_slice_in_dim(w_blend.T, pair, 2, 0),
        ],
        axis=0,
    )
    (sent,) = local_call(
        query_kernel,
        [((n, 2, rows, 4 * dim), BF16)],
        (
            core,
            exchanged(sent, "z"),
            gain_mix[None],
            w_query,
            w_key,
            w_value,
            other_query,
            gates,
        ),
        scalars=1,
    )
    got = exchanged(sent.reshape(2 * n, rows, 4 * dim), KVC).reshape(n, 2 * rows, 4 * dim)
    new_state, sent = local_call(
        state_kernel,
        [((seqs, dim, dim), F32), ((n, seqs, dim), BF16)],
        (
            got,
            state.reshape(seqs, dim, dim),
            decay_base[None],
            decay_shift[None],
            head_gain[None],
        ),
        scratch=(pltpu.VMEM((seqs, dim), F32),),
    )
    heads = exchanged(sent.reshape(2 * n, rows, dim), KVC).reshape(n, 2 * rows, dim)
    (sent,) = local_call(
        out_kernel, [(block, BF16)], (core, heads, w_out, other), scalars=1
    )

    sent, second = local_call(
        functools.partial(wide_kernel, units),
        [(wide, BF16), (tokens.shape, BF16)],
        (exchanged(sent, "z"), first, gain_post[None], later),
        far=(3,),
        scratch=(pltpu.VMEM((n, 2, 2 * units, width), BF16), pltpu.SemaphoreType.DMA((n,))),
        limit=24 << 20,
    )
    (hidden,) = local_call(
        functools.partial(hidden_kernel, units), [(narrow, BF16)], (exchanged(sent, KV),)
    )
    (result,) = local_call(
        functools.partial(last_kernel, units),
        [(tokens.shape, BF16)],
        (exchanged(hidden, KV), second, later),
        far=(2,),
        scratch=(pltpu.VMEM((n, 2, units, width), BF16), pltpu.SemaphoreType.DMA((n,))),
        limit=16 << 20,
    )
    return (result, new_state.reshape(state.shape))


def solution(mesh):
    finer = Mesh(mesh.devices.reshape(4, 4, mesh.shape["tp"] // 2, 2), ALL)
    in_specs = (
        P(TP, KV),
        P(KV, TP, None, None),
        P(KV),
        P(KV, TP),
        P(KV, TP),
        P(TP, KV),
        P(KV),
        P(KV, TP),
        P(KV, TP),
        P(KV, TP),
        P(KV, None),
        P(KV, None),
        P(TP),
        P(TP),
        P(),
        P(TP, KV),
        P(KV),
        P(KV, TP),
        P(KV, TP),
        P(TP, KV),
    )
    out_specs = (P(TP, KV), P(KV, TP, None, None))
    return jax.shard_map(
        on_device, mesh=finer, in_specs=in_specs, out_specs=out_specs, check_vma=False
    )
```

```python
import functools

import jax
import jax.numpy as jnp
from jax import lax
from jax.experimental import pallas as pl
from jax.experimental.pallas import tpu as pltpu
from jax.sharding import Mesh
from jax.sharding import PartitionSpec as P

D = 4096
EPS = 1e-06
KV = ("kv_0", "kv_1")
TP = ("z", "core")
KVC = ("kv_0", "kv_1", "core")
ALL = ("kv_0", "kv_1", "z", "core")
BF16 = jnp.bfloat16
F32 = jnp.float32


PAD = 384


def dot_nn(a, b):
    return jnp.dot(a, b, preferred_element_type=F32)


def dot_nt(a, b):
    return lax.dot_general(a, b, (((1,), (1,)), ((), ())), preferred_element_type=F32)


def exchanged(parts, axis):
    return lax.all_to_all(parts, axis, 0, 0, tiled=True)


def from_partner(x):
    return lax.ppermute(x, "core", [(0, 1), (1, 0)])


def local_call(kernel, shapes, args, *, scalars=0, far=(), scratch=(), limit=6 << 20):
    specs = [
        pl.BlockSpec(
            memory_space=pltpu.SMEM if i < scalars else pl.ANY if i in far else pltpu.VMEM
        )
        for i in range(len(args))
    ]
    outs = tuple(jax.ShapeDtypeStruct(shape, dtype) for shape, dtype in shapes)
    return pl.pallas_call(
        kernel,
        out_shape=outs,
        in_specs=specs,
        out_specs=tuple(pl.BlockSpec(memory_space=pltpu.VMEM) for _ in outs),
        scratch_shapes=list(scratch),
        compiler_params=pltpu.CompilerParams(vmem_limit_bytes=limit),
    )(*args)


def rows_of(ref):
    values = ref[...].astype(F32)
    return values.reshape(values.shape[0] * values.shape[1], values.shape[2])


def in_three(total):
    high = total.astype(BF16)
    rest = total - high.astype(F32)
    middle = rest.astype(BF16)
    return (high, middle, (rest - middle.astype(F32)).astype(BF16))


def scale_of(squares):
    return lax.rsqrt(squares / D + EPS)


def gate_up_kernel(rows_ref, gain_ref, gate_ref, up_ref, other_ref, out_ref):
    units = gate_ref.shape[0]
    n, rows, _ = rows_ref.shape
    stream = rows_of(rows_ref)
    scaled = (stream * gain_ref[...].astype(F32)).astype(BF16)
    weights = (gate_ref[...], other_ref[:units], up_ref[...], other_ref[units : 2 * units])
    for i, weight in enumerate(weights):
        out_ref[:, :, i * PAD + units : (i + 1) * PAD] = jnp.zeros((n, rows, PAD - units), BF16)
        product = dot_nt(scaled, weight).reshape(n, rows, units)
        out_ref[:, :, i * PAD : i * PAD + units] = product.astype(BF16)
    pieces = in_three(jnp.sum(stream * stream, axis=1, keepdims=True))
    for i, piece in enumerate(pieces):
        out_ref[:, :, units + i : units + i + 1] = (
            piece.astype(F32).reshape(n, rows, 1).astype(BF16)
        )


def hidden_kernel(units, parts_ref, out_ref):
    total = jnp.sum(parts_ref[...].astype(F32), axis=0)
    squares = jnp.sum(total[:, units : units + 3], axis=1, keepdims=True)
    factor = scale_of(squares)
    gate, up = factor * total[:, : 2 * PAD], factor * total[:, 2 * PAD :]
    hidden = (gate * jax.nn.sigmoid(gate) * up).astype(BF16)
    for i in range(out_ref.shape[0]):
        out_ref[i] = hidden


def down_kernel(hidden_ref, own_ref, other_ref, out_ref):
    units = own_ref.shape[0]
    hidden = rows_of(hidden_ref).astype(BF16)
    total = dot_nn(hidden[:, :units], own_ref[...])
    total += dot_nn(hidden[:, PAD : PAD + units], other_ref[2 * units : 3 * units])
    out_ref[...] = total.reshape(out_ref.shape).astype(BF16)


def first_kernel(parts_ref, own_ref, first_ref, out_ref):
    branch = jnp.sum(parts_ref[...].astype(F32), axis=0)
    first = (own_ref[...].astype(F32) + 0.5 * branch).astype(BF16)
    first_ref[...] = first
    for i in range(out_ref.shape[0]):
        out_ref[i] = first


def query_kernel(core_ref, rows_ref, gain_ref, q_ref, k_ref, v_ref, other_ref, gates_ref, out_ref):
    n, rows, _ = rows_ref.shape
    dim = q_ref.shape[1]
    stream = rows_of(rows_ref)
    scaled = (stream * gain_ref[...].astype(F32)).astype(BF16)
    is_first = core_ref[0] == 0
    for i, weight in enumerate((q_ref, k_ref, v_ref)):
        own = dot_nn(scaled, weight[...])
        other = dot_nn(scaled, other_ref[:, i * dim : (i + 1) * dim])
        for to, part in enumerate(
            (jnp.where(is_first, own, other), jnp.where(is_first, other, own))
        ):
            out_ref[:, to, :, i * dim : (i + 1) * dim] = part.reshape(n, rows, dim).astype(BF16)
    gates = dot_nt(scaled, gates_ref[...])
    pieces = in_three(jnp.sum(stream * stream, axis=1, keepdims=True))
    for to in range(2):
        columns = [gates[:, to : to + 1], gates[:, 2 + to : 3 + to]]
        columns += [piece.astype(F32) for piece in pieces]
        for i, column in enumerate(columns):
            at = 3 * dim + i
            out_ref[:, to, :, at : at + 1] = column.reshape(n, rows, 1).astype(BF16)


def state_kernel(
    parts_ref, state_ref, base_ref, shift_ref, head_gain_ref, state_out_ref, out_ref, held
):
    dim = state_ref.shape[2]
    got = jnp.sum(parts_ref[...].astype(F32), axis=0)
    squares = jnp.sum(got[:, 3 * dim + 2 : 3 * dim + 5], axis=1, keepdims=True)
    got = scale_of(squares) * got[:, : 3 * dim + 2]
    queries, keys, values = (got[:, i * dim : (i + 1) * dim] for i in range(3))
    decay_in, blend_in = got[:, 3 * dim : 3 * dim + 1], got[:, 3 * dim + 1 : 3 * dim + 2]

    def unit(v):
        return v * lax.rsqrt(jnp.sum(v * v, axis=1, keepdims=True) + EPS)

    queries, keys = unit(queries) * dim**-0.5, unit(keys)
    inner = decay_in + shift_ref[...]
    soft = jnp.maximum(inner, 0.0) + jnp.log1p(jnp.exp(-jnp.abs(inner)))
    rate = jnp.exp(-jnp.exp(base_ref[...]) * soft)
    beta = jax.nn.sigmoid(blend_in)
    queries_t, keys_t = queries.T, keys.T
    for b in range(state_ref.shape[0]):
        old = state_ref[b]
        key, query = keys_t[:, b : b + 1], queries_t[:, b : b + 1]
        rate_b = rate[b : b + 1]
        recalled = jnp.sum(key * old, axis=0, keepdims=True)
        correction = beta[b : b + 1] * (values[b : b + 1] - rate_b * recalled)
        new = rate_b * old + key * correction
        state_out_ref[b] = new
        held[b : b + 1] = jnp.sum(query * new, axis=0, keepdims=True)
    read = held[...]
    normed = read * lax.rsqrt(jnp.mean(read * read, axis=1, keepdims=True) + EPS)
    normed = (normed * head_gain_ref[...].astype(F32)).astype(BF16)
    for i in range(out_ref.shape[0]):
        out_ref[i] = normed


def out_kernel(core_ref, heads_ref, own_ref, other_ref, out_ref):
    n, both, dim = heads_ref.shape
    heads = heads_ref[...].astype(F32)
    zero = heads[:, : both // 2].reshape(n * both // 2, dim).astype(BF16)
    one = heads[:, both // 2 :].reshape(n * both // 2, dim).astype(BF16)
    from_zero, from_one = dot_nn, dot_nn
    is_first = core_ref[0] == 0
    own, other = own_ref[...], other_ref[other_ref.shape[0] - dim :]
    total = from_zero(zero, jnp.where(is_first, own, other))
    total += from_one(one, jnp.where(is_first, other, own))
    out_ref[...] = total.reshape(out_ref.shape).astype(BF16)


def wide_kernel(
    units, parts_ref, first_ref, gain_ref, weights_ref, out_ref, second_ref, held, sems
):
    n, rows, _ = out_ref.shape

    def copy(k):
        return pltpu.make_async_copy(
            weights_ref.at[pl.ds(2 * k, 2), pl.ds(0, 2 * units)], held.at[k], sems.at[k]
        )

    for k in range(n):
        copy(k).start()
    branch = jnp.sum(parts_ref[...].astype(F32), axis=0)
    second = (first_ref[...].astype(F32) + branch).astype(BF16)
    second_ref[...] = second
    stream = second.astype(F32)
    scaled = (stream * gain_ref[...].astype(F32)).astype(BF16)
    pieces = in_three(jnp.sum(stream * stream, axis=1, keepdims=True))
    for k in range(n):
        copy(k).wait()
        for i in range(4):
            out_ref[k, :, i * PAD + units : (i + 1) * PAD] = jnp.zeros((rows, PAD - units), BF16)
            weight = held[k, i % 2, (i // 2) * units : (i // 2 + 1) * units]
            out_ref[k, :, i * PAD : i * PAD + units] = dot_nt(scaled, weight).astype(BF16)
        for i, piece in enumerate(pieces):
            out_ref[k, :, units + i : units + i + 1] = piece


def last_kernel(units, hidden_ref, second_ref, weights_ref, out_ref):
    total = jnp.zeros(out_ref.shape, F32)
    for k in range(hidden_ref.shape[0]):
        for i in range(2):
            weight = weights_ref[2 * k + i, 2 * units : 3 * units]
            total += dot_nn(hidden_ref[k, :, i * PAD : i * PAD + units], weight)
    out_ref[...] = (second_ref[...].astype(F32) + 0.5 * total).astype(BF16)


def on_device(
    tokens,
    state,
    gain_pre,
    w_gate_pre,
    w_up_pre,
    w_down_pre,
    gain_mix,
    w_query,
    w_key,
    w_value,
    w_decay,
    w_blend,
    decay_base,
    decay_shift,
    head_gain,
    w_out,
    gain_post,
    w_gate_post,
    w_up_post,
    w_down_post,
):
    n = lax.axis_size(KV)
    rows, width = tokens.shape
    units = w_gate_pre.shape[1]
    seqs, _, dim, _ = state.shape
    core = lax.axis_index("core").reshape(1)
    block = (n, rows, width)
    wide = (n, rows, 4 * PAD)
    narrow = (n, rows, 2 * PAD)

    later = jnp.concatenate([w_gate_post.T, w_up_post.T, w_down_post], axis=0)
    later = lax.all_gather(later, TP, axis=0, tiled=False)

    gate_t, up_t = w_gate_pre.T, w_up_pre.T
    stream = exchanged(jnp.broadcast_to(tokens[None], block), "z")
    other = from_partner(jnp.concatenate([gate_t, up_t, w_down_pre, w_out], axis=0))
    (sent,) = local_call(
        gate_up_kernel, [(wide, BF16)], (stream, gain_pre[None], gate_t, up_t, other)
    )
    (hidden,) = local_call(
        functools.partial(hidden_kernel, units), [(narrow, BF16)], (exchanged(sent, KV),)
    )
    (sent,) = local_call(
        down_kernel, [(block, BF16)], (exchanged(hidden, KV), w_down_pre, other)
    )
    first, sent = local_call(
        first_kernel, [(tokens.shape, BF16), (block, BF16)], (exchanged(sent, "z"), tokens)
    )

    other_query = from_partner(jnp.concatenate([w_query, w_key, w_value], axis=1))
    pair = 2 * lax.axis_index("z")
    gates = jnp.concatenate(
        [
            lax.dynamic_slice_in_dim(w_decay.T, pair, 2, 0),
            lax.dynamic_slice_in_dim(w_blend.T, pair, 2, 0),
        ],
        axis=0,
    )
    (sent,) = local_call(
        query_kernel,
        [((n, 2, rows, 4 * dim), BF16)],
        (
            core,
            exchanged(sent, "z"),
            gain_mix[None],
            w_query,
            w_key,
            w_value,
            other_query,
            gates,
        ),
        scalars=1,
    )
    got = exchanged(sent.reshape(2 * n, rows, 4 * dim), KVC).reshape(n, 2 * rows, 4 * dim)
    new_state, sent = local_call(
        state_kernel,
        [((seqs, dim, dim), F32), ((n, seqs, dim), BF16)],
        (
            got,
            state.reshape(seqs, dim, dim),
            decay_base[None],
            decay_shift[None],
            head_gain[None],
        ),
        scratch=(pltpu.VMEM((seqs, dim), F32),),
    )
    heads = exchanged(sent.reshape(2 * n, rows, dim), KVC).reshape(n, 2 * rows, dim)
    (sent,) = local_call(
        out_kernel, [(block, BF16)], (core, heads, w_out, other), scalars=1
    )

    sent, second = local_call(
        functools.partial(wide_kernel, units),
        [(wide, BF16), (tokens.shape, BF16)],
        (exchanged(sent, "z"), first, gain_post[None], later),
        far=(3,),
        scratch=(pltpu.VMEM((n, 2, 2 * units, width), BF16), pltpu.SemaphoreType.DMA((n,))),
        limit=46 << 20,
    )
    (hidden,) = local_call(
        functools.partial(hidden_kernel, units), [(narrow, BF16)], (exchanged(sent, KV),)
    )
    (result,) = local_call(
        functools.partial(last_kernel, units),
        [(tokens.shape, BF16)],
        (exchanged(hidden, KV), second, later),
        limit=22 << 20,
    )
    return (result, new_state.reshape(state.shape))


def solution(mesh):
    finer = Mesh(mesh.devices.reshape(4, 4, mesh.shape["tp"] // 2, 2), ALL)
    in_specs = (
        P(TP, KV),
        P(KV, TP, None, None),
        P(KV),
        P(KV, TP),
        P(KV, TP),
        P(TP, KV),
        P(KV),
        P(KV, TP),
        P(KV, TP),
        P(KV, TP),
        P(KV, None),
        P(KV, None),
        P(TP),
        P(TP),
        P(),
        P(TP, KV),
        P(KV),
        P(KV, TP),
        P(KV, TP),
        P(TP, KV),
    )
    out_specs = (P(TP, KV), P(KV, TP, None, None))
    return jax.shard_map(
        on_device, mesh=finer, in_specs=in_specs, out_specs=out_specs, check_vma=False
    )
```

```python
import functools

import jax
import jax.numpy as jnp
from jax import lax
from jax.experimental import pallas as pl
from jax.experimental.pallas import tpu as pltpu
from jax.sharding import Mesh
from jax.sharding import PartitionSpec as P

D = 4096
EPS = 1e-06
KV = ("kv_0", "kv_1")
TP = ("z", "core")
KVC = ("kv_0", "kv_1", "core")
ALL = ("kv_0", "kv_1", "z", "core")
BF16 = jnp.bfloat16
F32 = jnp.float32


PAD = 384


def dot_nn(a, b):
    return jnp.dot(a, b, preferred_element_type=F32)


def dot_nt(a, b):
    return lax.dot_general(a, b, (((1,), (1,)), ((), ())), preferred_element_type=F32)


def exchanged(parts, axis):
    return lax.all_to_all(parts, axis, 0, 0, tiled=True)


def from_partner(x):
    return lax.ppermute(x, "core", [(0, 1), (1, 0)])


def local_call(kernel, shapes, args, *, scalars=0, far=(), scratch=(), limit=6 << 20):
    specs = [
        pl.BlockSpec(
            memory_space=pltpu.SMEM if i < scalars else pl.ANY if i in far else pltpu.VMEM
        )
        for i in range(len(args))
    ]
    outs = tuple(jax.ShapeDtypeStruct(shape, dtype) for shape, dtype in shapes)
    return pl.pallas_call(
        kernel,
        out_shape=outs,
        in_specs=specs,
        out_specs=tuple(pl.BlockSpec(memory_space=pltpu.VMEM) for _ in outs),
        scratch_shapes=list(scratch),
        compiler_params=pltpu.CompilerParams(vmem_limit_bytes=limit),
    )(*args)


def rows_of(ref):
    values = ref[...].astype(F32)
    return values.reshape(values.shape[0] * values.shape[1], values.shape[2])


def in_three(total):
    high = total.astype(BF16)
    rest = total - high.astype(F32)
    middle = rest.astype(BF16)
    return (high, middle, (rest - middle.astype(F32)).astype(BF16))


def scale_of(squares):
    return lax.rsqrt(squares / D + EPS)


def gate_up_kernel(rows_ref, gain_ref, gate_ref, up_ref, other_ref, out_ref):
    units = gate_ref.shape[0]
    n, rows, _ = rows_ref.shape
    stream = rows_of(rows_ref)
    scaled = (stream * gain_ref[...].astype(F32)).astype(BF16)
    weights = (gate_ref[...], other_ref[:units], up_ref[...], other_ref[units : 2 * units])
    for i, weight in enumerate(weights):
        out_ref[:, :, i * PAD + units : (i + 1) * PAD] = jnp.zeros((n, rows, PAD - units), BF16)
        product = dot_nt(scaled, weight).reshape(n, rows, units)
        out_ref[:, :, i * PAD : i * PAD + units] = product.astype(BF16)
    pieces = in_three(jnp.sum(stream * stream, axis=1, keepdims=True))
    for i, piece in enumerate(pieces):
        out_ref[:, :, units + i : units + i + 1] = (
            piece.astype(F32).reshape(n, rows, 1).astype(BF16)
        )


def hidden_kernel(units, parts_ref, out_ref):
    total = jnp.sum(parts_ref[...].astype(F32), axis=0)
    squares = jnp.sum(total[:, units : units + 3], axis=1, keepdims=True)
    factor = scale_of(squares)
    gate, up = factor * total[:, : 2 * PAD], factor * total[:, 2 * PAD :]
    hidden = (gate * jax.nn.sigmoid(gate) * up).astype(BF16)
    for i in range(out_ref.shape[0]):
        out_ref[i] = hidden


def down_kernel(hidden_ref, own_ref, other_ref, out_ref):
    units = own_ref.shape[0]
    hidden = rows_of(hidden_ref).astype(BF16)
    total = dot_nn(hidden[:, :units], own_ref[...])
    total += dot_nn(hidden[:, PAD : PAD + units], other_ref[2 * units : 3 * units])
    out_ref[...] = total.reshape(out_ref.shape).astype(BF16)


def first_kernel(parts_ref, own_ref, first_ref, out_ref):
    branch = jnp.sum(parts_ref[...].astype(F32), axis=0)
    first = (own_ref[...].astype(F32) + 0.5 * branch).astype(BF16)
    first_ref[...] = first
    for i in range(out_ref.shape[0]):
        out_ref[i] = first


def query_kernel(core_ref, rows_ref, gain_ref, q_ref, k_ref, v_ref, other_ref, gates_ref, out_ref):
    n, rows, _ = rows_ref.shape
    dim = q_ref.shape[1]
    stream = rows_of(rows_ref)
    scaled = (stream * gain_ref[...].astype(F32)).astype(BF16)
    is_first = core_ref[0] == 0
    for i, weight in enumerate((q_ref, k_ref, v_ref)):
        own = dot_nn(scaled, weight[...])
        other = dot_nn(scaled, other_ref[:, i * dim : (i + 1) * dim])
        for to, part in enumerate(
            (jnp.where(is_first, own, other), jnp.where(is_first, other, own))
        ):
            out_ref[:, to, :, i * dim : (i + 1) * dim] = part.reshape(n, rows, dim).astype(BF16)
    gates = dot_nt(scaled, gates_ref[...])
    pieces = in_three(jnp.sum(stream * stream, axis=1, keepdims=True))
    for to in range(2):
        columns = [gates[:, to : to + 1], gates[:, 2 + to : 3 + to]]
        columns += [piece.astype(F32) for piece in pieces]
        for i, column in enumerate(columns):
            at = 3 * dim + i
            out_ref[:, to, :, at : at + 1] = column.reshape(n, rows, 1).astype(BF16)


def state_kernel(
    parts_ref, state_ref, base_ref, shift_ref, head_gain_ref, state_out_ref, out_ref, held
):
    dim = state_ref.shape[2]
    got = jnp.sum(parts_ref[...].astype(F32), axis=0)
    squares = jnp.sum(got[:, 3 * dim + 2 : 3 * dim + 5], axis=1, keepdims=True)
    got = scale_of(squares) * got[:, : 3 * dim + 2]
    queries, keys, values = (got[:, i * dim : (i + 1) * dim] for i in range(3))
    decay_in, blend_in = got[:, 3 * dim : 3 * dim + 1], got[:, 3 * dim + 1 : 3 * dim + 2]

    def unit(v):
        return v * lax.rsqrt(jnp.sum(v * v, axis=1, keepdims=True) + EPS)

    queries, keys = unit(queries) * dim**-0.5, unit(keys)
    inner = decay_in + shift_ref[...]
    soft = jnp.maximum(inner, 0.0) + jnp.log1p(jnp.exp(-jnp.abs(inner)))
    rate = jnp.exp(-jnp.exp(base_ref[...]) * soft)
    beta = jax.nn.sigmoid(blend_in)
    queries_t, keys_t = queries.T, keys.T
    for b in range(state_ref.shape[0]):
        old = state_ref[b]
        key, query = keys_t[:, b : b + 1], queries_t[:, b : b + 1]
        rate_b = rate[b : b + 1]
        recalled = jnp.sum(key * old, axis=0, keepdims=True)
        correction = beta[b : b + 1] * (values[b : b + 1] - rate_b * recalled)
        new = rate_b * old + key * correction
        state_out_ref[b] = new
        held[b : b + 1] = jnp.sum(query * new, axis=0, keepdims=True)
    read = held[...]
    normed = read * lax.rsqrt(jnp.mean(read * read, axis=1, keepdims=True) + EPS)
    normed = (normed * head_gain_ref[...].astype(F32)).astype(BF16)
    for i in range(out_ref.shape[0]):
        out_ref[i] = normed


def out_kernel(core_ref, heads_ref, own_ref, other_ref, out_ref):
    n, both, dim = heads_ref.shape
    heads = heads_ref[...].astype(F32)
    zero = heads[:, : both // 2].reshape(n * both // 2, dim).astype(BF16)
    one = heads[:, both // 2 :].reshape(n * both // 2, dim).astype(BF16)
    from_zero, from_one = dot_nn, dot_nn
    is_first = core_ref[0] == 0
    own, other = own_ref[...], other_ref[other_ref.shape[0] - dim :]
    total = from_zero(zero, jnp.where(is_first, own, other))
    total += from_one(one, jnp.where(is_first, other, own))
    out_ref[...] = total.reshape(out_ref.shape).astype(BF16)


def wide_kernel(
    units, parts_ref, first_ref, gain_ref, weights_ref, out_ref, second_ref, held, sems
):
    n, rows, _ = out_ref.shape

    def copy(k):
        return pltpu.make_async_copy(weights_ref.at[pl.ds(2 * k, 2)], held.at[k], sems.at[k])

    for k in range(n):
        copy(k).start()
    branch = jnp.sum(parts_ref[...].astype(F32), axis=0)
    second = (first_ref[...].astype(F32) + branch).astype(BF16)
    second_ref[...] = second
    stream = second.astype(F32)
    scaled = (stream * gain_ref[...].astype(F32)).astype(BF16)
    pieces = in_three(jnp.sum(stream * stream, axis=1, keepdims=True))
    for k in range(n):
        for i in range(4):
            out_ref[k, :, i * PAD + units : (i + 1) * PAD] = jnp.zeros((rows, PAD - units), BF16)
        for i, piece in enumerate(pieces):
            out_ref[k, :, units + i : units + i + 1] = piece
    for k in range(n):
        copy(k).wait()
        for i in range(4):
            weight = held[k, i % 2, (i // 2) * units : (i // 2 + 1) * units]
            out_ref[k, :, i * PAD : i * PAD + units] = dot_nt(scaled, weight).astype(BF16)


def last_kernel(units, hidden_ref, second_ref, weights_ref, out_ref, held, sems):
    n = hidden_ref.shape[0]

    def copy(k):
        return pltpu.make_async_copy(weights_ref.at[pl.ds(2 * k, 2)], held.at[k], sems.at[k])

    for k in range(n):
        copy(k).start()
    total = jnp.zeros(out_ref.shape, F32)
    for k in range(n):
        copy(k).wait()
        for i in range(2):
            total += dot_nn(hidden_ref[k, :, i * PAD : i * PAD + units], held[k, i])
    out_ref[...] = (second_ref[...].astype(F32) + 0.5 * total).astype(BF16)


def on_device(
    tokens,
    state,
    gain_pre,
    w_gate_pre,
    w_up_pre,
    w_down_pre,
    gain_mix,
    w_query,
    w_key,
    w_value,
    w_decay,
    w_blend,
    decay_base,
    decay_shift,
    head_gain,
    w_out,
    gain_post,
    w_gate_post,
    w_up_post,
    w_down_post,
):
    n = lax.axis_size(KV)
    rows, width = tokens.shape
    units = w_gate_pre.shape[1]
    seqs, _, dim, _ = state.shape
    core = lax.axis_index("core").reshape(1)
    block = (n, rows, width)
    wide = (n, rows, 4 * PAD)
    narrow = (n, rows, 2 * PAD)

    gate_t, up_t = w_gate_pre.T, w_up_pre.T
    stream = exchanged(jnp.broadcast_to(tokens[None], block), "z")
    other = from_partner(jnp.concatenate([gate_t, up_t, w_down_pre, w_out], axis=0))
    wide_own = jnp.concatenate([w_gate_post.T, w_up_post.T], axis=0)
    wide_all = lax.all_gather(wide_own, TP, axis=0, tiled=False)
    down_all = lax.all_gather(w_down_post, TP, axis=0, tiled=False)
    (sent,) = local_call(
        gate_up_kernel, [(wide, BF16)], (stream, gain_pre[None], gate_t, up_t, other)
    )
    (hidden,) = local_call(
        functools.partial(hidden_kernel, units), [(narrow, BF16)], (exchanged(sent, KV),)
    )
    (sent,) = local_call(
        down_kernel, [(block, BF16)], (exchanged(hidden, KV), w_down_pre, other)
    )
    first, sent = local_call(
        first_kernel, [(tokens.shape, BF16), (block, BF16)], (exchanged(sent, "z"), tokens)
    )

    other_query = from_partner(jnp.concatenate([w_query, w_key, w_value], axis=1))
    pair = 2 * lax.axis_index("z")
    gates = jnp.concatenate(
        [
            lax.dynamic_slice_in_dim(w_decay.T, pair, 2, 0),
            lax.dynamic_slice_in_dim(w_blend.T, pair, 2, 0),
        ],
        axis=0,
    )
    (sent,) = local_call(
        query_kernel,
        [((n, 2, rows, 4 * dim), BF16)],
        (
            core,
            exchanged(sent, "z"),
            gain_mix[None],
            w_query,
            w_key,
            w_value,
            other_query,
            gates,
        ),
        scalars=1,
    )
    got = exchanged(sent.reshape(2 * n, rows, 4 * dim), KVC).reshape(n, 2 * rows, 4 * dim)
    new_state, sent = local_call(
        state_kernel,
        [((seqs, dim, dim), F32), ((n, seqs, dim), BF16)],
        (
            got,
            state.reshape(seqs, dim, dim),
            decay_base[None],
            decay_shift[None],
            head_gain[None],
        ),
        scratch=(pltpu.VMEM((seqs, dim), F32),),
    )
    heads = exchanged(sent.reshape(2 * n, rows, dim), KVC).reshape(n, 2 * rows, dim)
    heads, gain_last = lax.optimization_barrier((heads, gain_post[None]))
    (sent,) = local_call(
        out_kernel, [(block, BF16)], (core, heads, w_out, other), scalars=1
    )

    sent, second = local_call(
        functools.partial(wide_kernel, units),
        [(wide, BF16), (tokens.shape, BF16)],
        (exchanged(sent, "z"), first, gain_last, wide_all),
        far=(3,),
        scratch=(pltpu.VMEM((n, 2, 2 * units, width), BF16), pltpu.SemaphoreType.DMA((n,))),
        limit=46 << 20,
    )
    (hidden,) = local_call(
        functools.partial(hidden_kernel, units), [(narrow, BF16)], (exchanged(sent, KV),)
    )
    (result,) = local_call(
        functools.partial(last_kernel, units),
        [(tokens.shape, BF16)],
        (exchanged(hidden, KV), second, down_all),
        far=(2,),
        scratch=(pltpu.VMEM((n, 2, units, width), BF16), pltpu.SemaphoreType.DMA((n,))),
        limit=50 << 20,
    )
    return (result, new_state.reshape(state.shape))


def solution(mesh):
    finer = Mesh(mesh.devices.reshape(4, 4, mesh.shape["tp"] // 2, 2), ALL)
    in_specs = (
        P(TP, KV),
        P(KV, TP, None, None),
        P(KV),
        P(KV, TP),
        P(KV, TP),
        P(TP, KV),
        P(KV),
        P(KV, TP),
        P(KV, TP),
        P(KV, TP),
        P(KV, None),
        P(KV, None),
        P(TP),
        P(TP),
        P(),
        P(TP, KV),
        P(KV),
        P(KV, TP),
        P(KV, TP),
        P(TP, KV),
    )
    out_specs = (P(TP, KV), P(KV, TP, None, None))
    return jax.shard_map(
        on_device, mesh=finer, in_specs=in_specs, out_specs=out_specs, check_vma=False
    )
```

```python
import functools

import jax
import jax.numpy as jnp
from jax import lax
from jax.experimental import pallas as pl
from jax.experimental.pallas import tpu as pltpu
from jax.sharding import Mesh
from jax.sharding import PartitionSpec as P

D = 4096
EPS = 1e-06
KV = ("kv_0", "kv_1")
TP = ("z", "core")
KVC = ("kv_0", "kv_1", "core")
ALL = ("kv_0", "kv_1", "z", "core")
BF16 = jnp.bfloat16
F32 = jnp.float32


PAD = 384
AHEAD = 5


def dot_nn(a, b):
    return jnp.dot(a, b, preferred_element_type=F32)


def dot_nt(a, b):
    return lax.dot_general(a, b, (((1,), (1,)), ((), ())), preferred_element_type=F32)


def exchanged(parts, axis):
    return lax.all_to_all(parts, axis, 0, 0, tiled=True)


def from_partner(x):
    return lax.ppermute(x, "core", [(0, 1), (1, 0)])


def local_call(kernel, shapes, args, *, scalars=0, far=(), scratch=(), limit=6 << 20):
    specs = [
        pl.BlockSpec(
            memory_space=pltpu.SMEM if i < scalars else pl.ANY if i in far else pltpu.VMEM
        )
        for i in range(len(args))
    ]
    outs = tuple(jax.ShapeDtypeStruct(shape, dtype) for shape, dtype in shapes)
    return pl.pallas_call(
        kernel,
        out_shape=outs,
        in_specs=specs,
        out_specs=tuple(pl.BlockSpec(memory_space=pltpu.VMEM) for _ in outs),
        scratch_shapes=list(scratch),
        compiler_params=pltpu.CompilerParams(vmem_limit_bytes=limit),
    )(*args)


def rows_of(ref):
    values = ref[...].astype(F32)
    return values.reshape(values.shape[0] * values.shape[1], values.shape[2])


def in_three(total):
    high = total.astype(BF16)
    rest = total - high.astype(F32)
    middle = rest.astype(BF16)
    return (high, middle, (rest - middle.astype(F32)).astype(BF16))


def scale_of(squares):
    return lax.rsqrt(squares / D + EPS)


def gate_up_kernel(rows_ref, gain_ref, gate_ref, up_ref, other_ref, out_ref):
    units = gate_ref.shape[0]
    n, rows, _ = rows_ref.shape
    stream = rows_of(rows_ref)
    scaled = (stream * gain_ref[...].astype(F32)).astype(BF16)
    weights = (gate_ref[...], other_ref[:units], up_ref[...], other_ref[units : 2 * units])
    for i, weight in enumerate(weights):
        out_ref[:, :, i * PAD + units : (i + 1) * PAD] = jnp.zeros((n, rows, PAD - units), BF16)
        product = dot_nt(scaled, weight).reshape(n, rows, units)
        out_ref[:, :, i * PAD : i * PAD + units] = product.astype(BF16)
    pieces = in_three(jnp.sum(stream * stream, axis=1, keepdims=True))
    for i, piece in enumerate(pieces):
        out_ref[:, :, units + i : units + i + 1] = (
            piece.astype(F32).reshape(n, rows, 1).astype(BF16)
        )


def hidden_kernel(units, parts_ref, out_ref):
    total = jnp.sum(parts_ref[...].astype(F32), axis=0)
    squares = jnp.sum(total[:, units : units + 3], axis=1, keepdims=True)
    factor = scale_of(squares)
    gate, up = factor * total[:, : 2 * PAD], factor * total[:, 2 * PAD :]
    hidden = (gate * jax.nn.sigmoid(gate) * up).astype(BF16)
    for i in range(out_ref.shape[0]):
        out_ref[i] = hidden


def down_kernel(hidden_ref, own_ref, other_ref, out_ref):
    units = own_ref.shape[0]
    hidden = rows_of(hidden_ref).astype(BF16)
    total = dot_nn(hidden[:, :units], own_ref[...])
    total += dot_nn(hidden[:, PAD : PAD + units], other_ref[2 * units : 3 * units])
    out_ref[...] = total.reshape(out_ref.shape).astype(BF16)


def first_kernel(parts_ref, own_ref, first_ref, out_ref):
    branch = jnp.sum(parts_ref[...].astype(F32), axis=0)
    first = (own_ref[...].astype(F32) + 0.5 * branch).astype(BF16)
    first_ref[...] = first
    for i in range(out_ref.shape[0]):
        out_ref[i] = first


def query_kernel(core_ref, rows_ref, gain_ref, q_ref, k_ref, v_ref, other_ref, gates_ref, out_ref):
    n, rows, _ = rows_ref.shape
    dim = q_ref.shape[1]
    stream = rows_of(rows_ref)
    scaled = (stream * gain_ref[...].astype(F32)).astype(BF16)
    is_first = core_ref[0] == 0
    for i, weight in enumerate((q_ref, k_ref, v_ref)):
        own = dot_nn(scaled, weight[...])
        other = dot_nn(scaled, other_ref[:, i * dim : (i + 1) * dim])
        for to, part in enumerate(
            (jnp.where(is_first, own, other), jnp.where(is_first, other, own))
        ):
            out_ref[:, to, :, i * dim : (i + 1) * dim] = part.reshape(n, rows, dim).astype(BF16)
    gates = dot_nt(scaled, gates_ref[...])
    pieces = in_three(jnp.sum(stream * stream, axis=1, keepdims=True))
    for to in range(2):
        columns = [gates[:, to : to + 1], gates[:, 2 + to : 3 + to]]
        columns += [piece.astype(F32) for piece in pieces]
        for i, column in enumerate(columns):
            at = 3 * dim + i
            out_ref[:, to, :, at : at + 1] = column.reshape(n, rows, 1).astype(BF16)


def state_kernel(
    parts_ref, state_ref, base_ref, shift_ref, head_gain_ref, state_out_ref, out_ref, held
):
    dim = state_ref.shape[2]
    got = jnp.sum(parts_ref[...].astype(F32), axis=0)
    squares = jnp.sum(got[:, 3 * dim + 2 : 3 * dim + 5], axis=1, keepdims=True)
    got = scale_of(squares) * got[:, : 3 * dim + 2]
    queries, keys, values = (got[:, i * dim : (i + 1) * dim] for i in range(3))
    decay_in, blend_in = got[:, 3 * dim : 3 * dim + 1], got[:, 3 * dim + 1 : 3 * dim + 2]

    def unit(v):
        return v * lax.rsqrt(jnp.sum(v * v, axis=1, keepdims=True) + EPS)

    queries, keys = unit(queries) * dim**-0.5, unit(keys)
    inner = decay_in + shift_ref[...]
    soft = jnp.maximum(inner, 0.0) + jnp.log1p(jnp.exp(-jnp.abs(inner)))
    rate = jnp.exp(-jnp.exp(base_ref[...]) * soft)
    beta = jax.nn.sigmoid(blend_in)
    queries_t, keys_t = queries.T, keys.T
    for b in range(state_ref.shape[0]):
        old = state_ref[b]
        key, query = keys_t[:, b : b + 1], queries_t[:, b : b + 1]
        rate_b = rate[b : b + 1]
        recalled = jnp.sum(key * old, axis=0, keepdims=True)
        correction = beta[b : b + 1] * (values[b : b + 1] - rate_b * recalled)
        new = rate_b * old + key * correction
        state_out_ref[b] = new
        held[b : b + 1] = jnp.sum(query * new, axis=0, keepdims=True)
    read = held[...]
    normed = read * lax.rsqrt(jnp.mean(read * read, axis=1, keepdims=True) + EPS)
    normed = (normed * head_gain_ref[...].astype(F32)).astype(BF16)
    for i in range(out_ref.shape[0]):
        out_ref[i] = normed


def out_kernel(core_ref, heads_ref, own_ref, other_ref, out_ref):
    n, both, dim = heads_ref.shape
    heads = heads_ref[...].astype(F32)
    zero = heads[:, : both // 2].reshape(n * both // 2, dim).astype(BF16)
    one = heads[:, both // 2 :].reshape(n * both // 2, dim).astype(BF16)
    from_zero, from_one = dot_nn, dot_nn
    is_first = core_ref[0] == 0
    own, other = own_ref[...], other_ref[other_ref.shape[0] - dim :]
    total = from_zero(zero, jnp.where(is_first, own, other))
    total += from_one(one, jnp.where(is_first, other, own))
    out_ref[...] = total.reshape(out_ref.shape).astype(BF16)


def wide_kernel(
    units, parts_ref, first_ref, gain_ref, weights_ref, out_ref, second_ref, held, sems
):
    n, rows, _ = out_ref.shape

    def copy(k):
        return pltpu.make_async_copy(
            weights_ref.at[pl.ds(2 * k, 2), pl.ds(0, 2 * units)], held.at[k], sems.at[k]
        )

    for k in range(AHEAD):
        copy(k).start()
    branch = jnp.sum(parts_ref[...].astype(F32), axis=0)
    second = (first_ref[...].astype(F32) + branch).astype(BF16)
    second_ref[...] = second
    stream = second.astype(F32)
    scaled = (stream * gain_ref[...].astype(F32)).astype(BF16)
    pieces = in_three(jnp.sum(stream * stream, axis=1, keepdims=True))
    for k in range(n):
        for i in range(4):
            out_ref[k, :, i * PAD + units : (i + 1) * PAD] = jnp.zeros((rows, PAD - units), BF16)
        for i, piece in enumerate(pieces):
            out_ref[k, :, units + i : units + i + 1] = piece
    for k in range(n):
        copy(k).wait()
        if k + AHEAD < n:
            copy(k + AHEAD).start()
        for i in range(4):
            weight = held[k, i % 2, (i // 2) * units : (i // 2 + 1) * units]
            out_ref[k, :, i * PAD : i * PAD + units] = dot_nt(scaled, weight).astype(BF16)


def last_kernel(units, hidden_ref, second_ref, weights_ref, out_ref):
    total = jnp.zeros(out_ref.shape, F32)
    for k in range(hidden_ref.shape[0]):
        for i in range(2):
            weight = weights_ref[2 * k + i, 2 * units : 3 * units]
            total += dot_nn(hidden_ref[k, :, i * PAD : i * PAD + units], weight)
    out_ref[...] = (second_ref[...].astype(F32) + 0.5 * total).astype(BF16)


def on_device(
    tokens,
    state,
    gain_pre,
    w_gate_pre,
    w_up_pre,
    w_down_pre,
    gain_mix,
    w_query,
    w_key,
    w_value,
    w_decay,
    w_blend,
    decay_base,
    decay_shift,
    head_gain,
    w_out,
    gain_post,
    w_gate_post,
    w_up_post,
    w_down_post,
):
    n = lax.axis_size(KV)
    rows, width = tokens.shape
    units = w_gate_pre.shape[1]
    seqs, _, dim, _ = state.shape
    core = lax.axis_index("core").reshape(1)
    block = (n, rows, width)
    wide = (n, rows, 4 * PAD)
    narrow = (n, rows, 2 * PAD)

    gate_t, up_t = w_gate_pre.T, w_up_pre.T
    stream = exchanged(jnp.broadcast_to(tokens[None], block), "z")
    other = from_partner(jnp.concatenate([gate_t, up_t, w_down_pre, w_out], axis=0))
    later = jnp.concatenate([w_gate_post.T, w_up_post.T, w_down_post], axis=0)
    later = lax.all_gather(later, TP, axis=0, tiled=False)
    (sent,) = local_call(
        gate_up_kernel, [(wide, BF16)], (stream, gain_pre[None], gate_t, up_t, other)
    )
    (hidden,) = local_call(
        functools.partial(hidden_kernel, units), [(narrow, BF16)], (exchanged(sent, KV),)
    )
    (sent,) = local_call(
        down_kernel, [(block, BF16)], (exchanged(hidden, KV), w_down_pre, other)
    )
    first, sent = local_call(
        first_kernel, [(tokens.shape, BF16), (block, BF16)], (exchanged(sent, "z"), tokens)
    )

    other_query = from_partner(jnp.concatenate([w_query, w_key, w_value], axis=1))
    pair = 2 * lax.axis_index("z")
    gates = jnp.concatenate(
        [
            lax.dynamic_slice_in_dim(w_decay.T, pair, 2, 0),
            lax.dynamic_slice_in_dim(w_blend.T, pair, 2, 0),
        ],
        axis=0,
    )
    (sent,) = local_call(
        query_kernel,
        [((n, 2, rows, 4 * dim), BF16)],
        (
            core,
            exchanged(sent, "z"),
            gain_mix[None],
            w_query,
            w_key,
            w_value,
            other_query,
            gates,
        ),
        scalars=1,
    )
    got = exchanged(sent.reshape(2 * n, rows, 4 * dim), KVC).reshape(n, 2 * rows, 4 * dim)
    new_state, sent = local_call(
        state_kernel,
        [((seqs, dim, dim), F32), ((n, seqs, dim), BF16)],
        (
            got,
            state.reshape(seqs, dim, dim),
            decay_base[None],
            decay_shift[None],
            head_gain[None],
        ),
        scratch=(pltpu.VMEM((seqs, dim), F32),),
    )
    heads = exchanged(sent.reshape(2 * n, rows, dim), KVC).reshape(n, 2 * rows, dim)
    (sent,) = local_call(
        out_kernel, [(block, BF16)], (core, heads, w_out, other), scalars=1
    )

    sent, second = local_call(
        functools.partial(wide_kernel, units),
        [(wide, BF16), (tokens.shape, BF16)],
        (exchanged(sent, "z"), first, gain_post[None], later),
        far=(3,),
        scratch=(pltpu.VMEM((n, 2, 2 * units, width), BF16), pltpu.SemaphoreType.DMA((n,))),
        limit=46 << 20,
    )
    (hidden,) = local_call(
        functools.partial(hidden_kernel, units), [(narrow, BF16)], (exchanged(sent, KV),)
    )
    (result,) = local_call(
        functools.partial(last_kernel, units),
        [(tokens.shape, BF16)],
        (exchanged(hidden, KV), second, later),
        limit=22 << 20,
    )
    return (result, new_state.reshape(state.shape))


def solution(mesh):
    finer = Mesh(mesh.devices.reshape(4, 4, mesh.shape["tp"] // 2, 2), ALL)
    in_specs = (
        P(TP, KV),
        P(KV, TP, None, None),
        P(KV),
        P(KV, TP),
        P(KV, TP),
        P(TP, KV),
        P(KV),
        P(KV, TP),
        P(KV, TP),
        P(KV, TP),
        P(KV, None),
        P(KV, None),
        P(TP),
        P(TP),
        P(),
        P(TP, KV),
        P(KV),
        P(KV, TP),
        P(KV, TP),
        P(TP, KV),
    )
    out_specs = (P(TP, KV), P(KV, TP, None, None))
    return jax.shard_map(
        on_device, mesh=finer, in_specs=in_specs, out_specs=out_specs, check_vma=False
    )
```

```python
import functools

import jax
import jax.numpy as jnp
from jax import lax
from jax.experimental import pallas as pl
from jax.experimental.pallas import tpu as pltpu
from jax.sharding import Mesh
from jax.sharding import PartitionSpec as P

D = 4096
EPS = 1e-06
KV = ("kv_0", "kv_1")
TP = ("z", "core")
KVC = ("kv_0", "kv_1", "core")
ALL = ("kv_0", "kv_1", "z", "core")
BF16 = jnp.bfloat16
F32 = jnp.float32


PAD = 384
AHEAD = 5


def dot_nn(a, b):
    return jnp.dot(a, b, preferred_element_type=F32)


def dot_nt(a, b):
    return lax.dot_general(a, b, (((1,), (1,)), ((), ())), preferred_element_type=F32)


def exchanged(parts, axis):
    return lax.all_to_all(parts, axis, 0, 0, tiled=True)


def from_partner(x):
    return lax.ppermute(x, "core", [(0, 1), (1, 0)])


def local_call(kernel, shapes, args, *, scalars=0, far=(), scratch=(), limit=6 << 20, cost=None):
    specs = [
        pl.BlockSpec(
            memory_space=pltpu.SMEM if i < scalars else pl.ANY if i in far else pltpu.VMEM
        )
        for i in range(len(args))
    ]
    outs = tuple(jax.ShapeDtypeStruct(shape, dtype) for shape, dtype in shapes)
    return pl.pallas_call(
        kernel,
        out_shape=outs,
        in_specs=specs,
        out_specs=tuple(pl.BlockSpec(memory_space=pltpu.VMEM) for _ in outs),
        scratch_shapes=list(scratch),
        compiler_params=pltpu.CompilerParams(vmem_limit_bytes=limit),
        cost_estimate=cost,
    )(*args)


def rows_of(ref):
    values = ref[...].astype(F32)
    return values.reshape(values.shape[0] * values.shape[1], values.shape[2])


def in_three(total):
    high = total.astype(BF16)
    rest = total - high.astype(F32)
    middle = rest.astype(BF16)
    return (high, middle, (rest - middle.astype(F32)).astype(BF16))


def scale_of(squares):
    return lax.rsqrt(squares / D + EPS)


def gate_up_kernel(rows_ref, gain_ref, gate_ref, up_ref, other_ref, out_ref):
    units = gate_ref.shape[0]
    n, rows, _ = rows_ref.shape
    stream = rows_of(rows_ref)
    scaled = (stream * gain_ref[...].astype(F32)).astype(BF16)
    weights = (gate_ref[...], other_ref[:units], up_ref[...], other_ref[units : 2 * units])
    for i, weight in enumerate(weights):
        out_ref[:, :, i * PAD + units : (i + 1) * PAD] = jnp.zeros((n, rows, PAD - units), BF16)
        product = dot_nt(scaled, weight).reshape(n, rows, units)
        out_ref[:, :, i * PAD : i * PAD + units] = product.astype(BF16)
    pieces = in_three(jnp.sum(stream * stream, axis=1, keepdims=True))
    for i, piece in enumerate(pieces):
        out_ref[:, :, units + i : units + i + 1] = (
            piece.astype(F32).reshape(n, rows, 1).astype(BF16)
        )


def hidden_kernel(units, parts_ref, *refs):
    out_ref = refs[-1]
    total = jnp.sum(parts_ref[...].astype(F32), axis=0)
    squares = jnp.sum(total[:, units : units + 3], axis=1, keepdims=True)
    factor = scale_of(squares)
    gate, up = factor * total[:, : 2 * PAD], factor * total[:, 2 * PAD :]
    hidden = (gate * jax.nn.sigmoid(gate) * up).astype(BF16)
    for i in range(out_ref.shape[0]):
        out_ref[i] = hidden


def down_kernel(hidden_ref, own_ref, other_ref, out_ref):
    units = own_ref.shape[0]
    hidden = rows_of(hidden_ref).astype(BF16)
    total = dot_nn(hidden[:, :units], own_ref[...])
    total += dot_nn(hidden[:, PAD : PAD + units], other_ref[2 * units : 3 * units])
    out_ref[...] = total.reshape(out_ref.shape).astype(BF16)


def first_kernel(parts_ref, own_ref, first_ref, out_ref):
    branch = jnp.sum(parts_ref[...].astype(F32), axis=0)
    first = (own_ref[...].astype(F32) + 0.5 * branch).astype(BF16)
    first_ref[...] = first
    for i in range(out_ref.shape[0]):
        out_ref[i] = first


def query_kernel(core_ref, rows_ref, gain_ref, q_ref, k_ref, v_ref, other_ref, gates_ref, out_ref):
    n, rows, _ = rows_ref.shape
    dim = q_ref.shape[1]
    stream = rows_of(rows_ref)
    scaled = (stream * gain_ref[...].astype(F32)).astype(BF16)
    is_first = core_ref[0] == 0
    for i, weight in enumerate((q_ref, k_ref, v_ref)):
        own = dot_nn(scaled, weight[...])
        other = dot_nn(scaled, other_ref[:, i * dim : (i + 1) * dim])
        for to, part in enumerate(
            (jnp.where(is_first, own, other), jnp.where(is_first, other, own))
        ):
            out_ref[:, to, :, i * dim : (i + 1) * dim] = part.reshape(n, rows, dim).astype(BF16)
    gates = dot_nt(scaled, gates_ref[...])
    pieces = in_three(jnp.sum(stream * stream, axis=1, keepdims=True))
    for to in range(2):
        columns = [gates[:, to : to + 1], gates[:, 2 + to : 3 + to]]
        columns += [piece.astype(F32) for piece in pieces]
        for i, column in enumerate(columns):
            at = 3 * dim + i
            out_ref[:, to, :, at : at + 1] = column.reshape(n, rows, 1).astype(BF16)


def read_kernel(
    parts_ref,
    state_ref,
    base_ref,
    shift_ref,
    head_gain_ref,
    keys_ref,
    rate_ref,
    correction_ref,
    out_ref,
    recalled,
    queried,
):
    dim = state_ref.shape[2]
    got = jnp.sum(parts_ref[...].astype(F32), axis=0)
    squares = jnp.sum(got[:, 3 * dim + 2 : 3 * dim + 5], axis=1, keepdims=True)
    got = scale_of(squares) * got[:, : 3 * dim + 2]
    queries, keys, values = (got[:, i * dim : (i + 1) * dim] for i in range(3))
    decay_in, blend_in = got[:, 3 * dim : 3 * dim + 1], got[:, 3 * dim + 1 : 3 * dim + 2]

    def unit(v):
        return v * lax.rsqrt(jnp.sum(v * v, axis=1, keepdims=True) + EPS)

    queries, keys = unit(queries) * dim**-0.5, unit(keys)
    inner = decay_in + shift_ref[...]
    soft = jnp.maximum(inner, 0.0) + jnp.log1p(jnp.exp(-jnp.abs(inner)))
    rate = jnp.exp(-jnp.exp(base_ref[...]) * soft)
    beta = jax.nn.sigmoid(blend_in)
    queries_t, keys_t = queries.T, keys.T
    for b in range(state_ref.shape[0]):
        old = state_ref[b]
        recalled[b : b + 1] = jnp.sum(keys_t[:, b : b + 1] * old, axis=0, keepdims=True)
        queried[b : b + 1] = jnp.sum(queries_t[:, b : b + 1] * old, axis=0, keepdims=True)
    correction = beta * (values - rate * recalled[...])
    read = rate * queried[...] + jnp.sum(keys * queries, axis=1, keepdims=True) * correction
    normed = read * lax.rsqrt(jnp.mean(read * read, axis=1, keepdims=True) + EPS)
    normed = (normed * head_gain_ref[...].astype(F32)).astype(BF16)
    for i in range(out_ref.shape[0]):
        out_ref[i] = normed
    keys_ref[...] = keys_t
    rate_ref[...] = rate
    correction_ref[...] = correction


def state_kernel(state_ref, keys_ref, rate_ref, correction_ref, out_ref):
    keys_t, rate, correction = keys_ref[...], rate_ref[...], correction_ref[...]
    for b in range(state_ref.shape[0]):
        new = rate[b : b + 1] * state_ref[b] + keys_t[:, b : b + 1] * correction[b : b + 1]
        out_ref[b] = new


def out_kernel(core_ref, heads_ref, own_ref, other_ref, out_ref):
    n, both, dim = heads_ref.shape
    heads = heads_ref[...].astype(F32)
    zero = heads[:, : both // 2].reshape(n * both // 2, dim).astype(BF16)
    one = heads[:, both // 2 :].reshape(n * both // 2, dim).astype(BF16)
    from_zero, from_one = dot_nn, dot_nn
    is_first = core_ref[0] == 0
    own, other = own_ref[...], other_ref[other_ref.shape[0] - dim :]
    total = from_zero(zero, jnp.where(is_first, own, other))
    total += from_one(one, jnp.where(is_first, other, own))
    out_ref[...] = total.reshape(out_ref.shape).astype(BF16)


def wide_kernel(
    units, parts_ref, first_ref, gain_ref, weights_ref, out_ref, second_ref, held, sems
):
    n, rows, _ = out_ref.shape

    def copy(k):
        return pltpu.make_async_copy(
            weights_ref.at[pl.ds(2 * k, 2), pl.ds(0, 2 * units)], held.at[k], sems.at[k]
        )

    for k in range(AHEAD):
        copy(k).start()
    branch = jnp.sum(parts_ref[...].astype(F32), axis=0)
    second = (first_ref[...].astype(F32) + branch).astype(BF16)
    second_ref[...] = second
    stream = second.astype(F32)
    scaled = (stream * gain_ref[...].astype(F32)).astype(BF16)
    pieces = in_three(jnp.sum(stream * stream, axis=1, keepdims=True))
    for k in range(n):
        for i in range(4):
            out_ref[k, :, i * PAD + units : (i + 1) * PAD] = jnp.zeros((rows, PAD - units), BF16)
        for i, piece in enumerate(pieces):
            out_ref[k, :, units + i : units + i + 1] = piece
    for k in range(n):
        copy(k).wait()
        if k + AHEAD < n:
            copy(k + AHEAD).start()
        for i in range(4):
            weight = held[k, i % 2, (i // 2) * units : (i // 2 + 1) * units]
            out_ref[k, :, i * PAD : i * PAD + units] = dot_nt(scaled, weight).astype(BF16)


def last_kernel(units, hidden_ref, second_ref, weights_ref, out_ref):
    total = jnp.zeros(out_ref.shape, F32)
    for k in range(hidden_ref.shape[0]):
        for i in range(2):
            weight = weights_ref[2 * k + i, 2 * units : 3 * units]
            total += dot_nn(hidden_ref[k, :, i * PAD : i * PAD + units], weight)
    out_ref[...] = (second_ref[...].astype(F32) + 0.5 * total).astype(BF16)


def on_device(
    tokens,
    state,
    gain_pre,
    w_gate_pre,
    w_up_pre,
    w_down_pre,
    gain_mix,
    w_query,
    w_key,
    w_value,
    w_decay,
    w_blend,
    decay_base,
    decay_shift,
    head_gain,
    w_out,
    gain_post,
    w_gate_post,
    w_up_post,
    w_down_post,
):
    n = lax.axis_size(KV)
    rows, width = tokens.shape
    units = w_gate_pre.shape[1]
    seqs, _, dim, _ = state.shape
    core = lax.axis_index("core").reshape(1)
    block = (n, rows, width)
    wide = (n, rows, 4 * PAD)
    narrow = (n, rows, 2 * PAD)

    later = jnp.concatenate([w_gate_post.T, w_up_post.T, w_down_post], axis=0)
    later = lax.all_gather(later, TP, axis=0, tiled=False)

    gate_t, up_t = w_gate_pre.T, w_up_pre.T
    stream = exchanged(jnp.broadcast_to(tokens[None], block), "z")
    other = from_partner(jnp.concatenate([gate_t, up_t, w_down_pre, w_out], axis=0))
    (sent,) = local_call(
        gate_up_kernel, [(wide, BF16)], (stream, gain_pre[None], gate_t, up_t, other)
    )
    (hidden,) = local_call(
        functools.partial(hidden_kernel, units), [(narrow, BF16)], (exchanged(sent, KV),)
    )
    (sent,) = local_call(
        down_kernel, [(block, BF16)], (exchanged(hidden, KV), w_down_pre, other)
    )
    first, sent = local_call(
        first_kernel, [(tokens.shape, BF16), (block, BF16)], (exchanged(sent, "z"), tokens)
    )

    other_query = from_partner(jnp.concatenate([w_query, w_key, w_value], axis=1))
    pair = 2 * lax.axis_index("z")
    gates = jnp.concatenate(
        [
            lax.dynamic_slice_in_dim(w_decay.T, pair, 2, 0),
            lax.dynamic_slice_in_dim(w_blend.T, pair, 2, 0),
        ],
        axis=0,
    )
    (sent,) = local_call(
        query_kernel,
        [((n, 2, rows, 4 * dim), BF16)],
        (
            core,
            exchanged(sent, "z"),
            gain_mix[None],
            w_query,
            w_key,
            w_value,
            other_query,
            gates,
        ),
        scalars=1,
    )
    got = exchanged(sent.reshape(2 * n, rows, 4 * dim), KVC).reshape(n, 2 * rows, 4 * dim)
    held = state.reshape(seqs, dim, dim)
    keys_t, rate, correction, sent = local_call(
        read_kernel,
        [((dim, seqs), F32), ((seqs, 1), F32), ((seqs, dim), F32), ((n, seqs, dim), BF16)],
        (got, held, decay_base[None], decay_shift[None], head_gain[None]),
        scratch=(pltpu.VMEM((seqs, dim), F32), pltpu.VMEM((seqs, dim), F32)),
    )
    (new_state,) = local_call(
        state_kernel,
        [((seqs, dim, dim), F32)],
        (held, keys_t, rate, correction),
        cost=pl.CostEstimate(flops=1 << 28, bytes_accessed=8 * held.size, transcendentals=0),
    )
    heads = exchanged(sent.reshape(2 * n, rows, dim), KVC).reshape(n, 2 * rows, dim)
    heads, new_state = lax.optimization_barrier((heads, new_state))
    (sent,) = local_call(
        out_kernel, [(block, BF16)], (core, heads, w_out, other), scalars=1
    )

    sent, second = local_call(
        functools.partial(wide_kernel, units),
        [(wide, BF16), (tokens.shape, BF16)],
        (exchanged(sent, "z"), first, gain_post[None], later),
        far=(3,),
        scratch=(pltpu.VMEM((n, 2, 2 * units, width), BF16), pltpu.SemaphoreType.DMA((n,))),
        limit=46 << 20,
    )
    (hidden,) = local_call(
        functools.partial(hidden_kernel, units),
        [(narrow, BF16)],
        (exchanged(sent, KV), *(later,) * 4),
        far=range(1, 5),
        limit=40 << 20,
    )
    (result,) = local_call(
        functools.partial(last_kernel, units),
        [(tokens.shape, BF16)],
        (exchanged(hidden, KV), second, later),
        limit=22 << 20,
    )
    return (result, new_state.reshape(state.shape))


def solution(mesh):
    finer = Mesh(mesh.devices.reshape(4, 4, mesh.shape["tp"] // 2, 2), ALL)
    in_specs = (
        P(TP, KV),
        P(KV, TP, None, None),
        P(KV),
        P(KV, TP),
        P(KV, TP),
        P(TP, KV),
        P(KV),
        P(KV, TP),
        P(KV, TP),
        P(KV, TP),
        P(KV, None),
        P(KV, None),
        P(TP),
        P(TP),
        P(),
        P(TP, KV),
        P(KV),
        P(KV, TP),
        P(KV, TP),
        P(TP, KV),
    )
    out_specs = (P(TP, KV), P(KV, TP, None, None))
    return jax.shard_map(
        on_device, mesh=finer, in_specs=in_specs, out_specs=out_specs, check_vma=False
    )
```

```python
import functools

import jax
import jax.numpy as jnp
from jax import lax
from jax.experimental import pallas as pl
from jax.experimental.pallas import tpu as pltpu
from jax.sharding import Mesh
from jax.sharding import PartitionSpec as P

D = 4096
EPS = 1e-06
KV = ("kv_0", "kv_1")
TP = ("z", "core")
KVC = ("kv_0", "kv_1", "core")
ALL = ("kv_0", "kv_1", "z", "core")
BF16 = jnp.bfloat16
F32 = jnp.float32


PAD = 384
AHEAD = 5


def dot_nn(a, b):
    return jnp.dot(a, b, preferred_element_type=F32)


def dot_nt(a, b):
    return lax.dot_general(a, b, (((1,), (1,)), ((), ())), preferred_element_type=F32)


def exchanged(parts, axis):
    return lax.all_to_all(parts, axis, 0, 0, tiled=True)


def from_partner(x):
    return lax.ppermute(x, "core", [(0, 1), (1, 0)])


def local_call(kernel, shapes, args, *, scalars=0, far=(), scratch=(), limit=6 << 20, cost=None):
    specs = [
        pl.BlockSpec(
            memory_space=pltpu.SMEM if i < scalars else pl.ANY if i in far else pltpu.VMEM
        )
        for i in range(len(args))
    ]
    outs = tuple(jax.ShapeDtypeStruct(shape, dtype) for shape, dtype in shapes)
    return pl.pallas_call(
        kernel,
        out_shape=outs,
        in_specs=specs,
        out_specs=tuple(pl.BlockSpec(memory_space=pltpu.VMEM) for _ in outs),
        scratch_shapes=list(scratch),
        compiler_params=pltpu.CompilerParams(vmem_limit_bytes=limit),
        cost_estimate=cost,
    )(*args)


def join_kernel(*refs):
    parts, out_ref, sems = refs[:-2], refs[-2], refs[-1]
    copies, at = [], 0
    for i, part in enumerate(parts):
        rows = part.shape[0]
        copies.append(pltpu.make_async_copy(part, out_ref.at[pl.ds(at, rows)], sems.at[i]))
        copies[-1].start()
        at += rows
    for copy in copies:
        copy.wait()


def joined(*parts):
    rows, width = sum(part.shape[0] for part in parts), parts[0].shape[1]
    return pl.pallas_call(
        join_kernel,
        out_shape=jax.ShapeDtypeStruct((rows, width), parts[0].dtype),
        in_specs=[pl.BlockSpec(memory_space=pl.ANY)] * len(parts),
        out_specs=pl.BlockSpec(memory_space=pl.ANY),
        scratch_shapes=[pltpu.SemaphoreType.DMA((len(parts),))],
    )(*parts)


def rows_of(ref):
    values = ref[...].astype(F32)
    return values.reshape(values.shape[0] * values.shape[1], values.shape[2])


def in_three(total):
    high = total.astype(BF16)
    rest = total - high.astype(F32)
    middle = rest.astype(BF16)
    return (high, middle, (rest - middle.astype(F32)).astype(BF16))


def scale_of(squares):
    return lax.rsqrt(squares / D + EPS)


def gate_up_kernel(rows_ref, gain_ref, gate_ref, up_ref, other_ref, out_ref):
    units = gate_ref.shape[0]
    n, rows, _ = rows_ref.shape
    stream = rows_of(rows_ref)
    scaled = (stream * gain_ref[...].astype(F32)).astype(BF16)
    weights = (gate_ref[...], other_ref[:units], up_ref[...], other_ref[units : 2 * units])
    for i, weight in enumerate(weights):
        out_ref[:, :, i * PAD + units : (i + 1) * PAD] = jnp.zeros((n, rows, PAD - units), BF16)
        product = dot_nt(scaled, weight).reshape(n, rows, units)
        out_ref[:, :, i * PAD : i * PAD + units] = product.astype(BF16)
    pieces = in_three(jnp.sum(stream * stream, axis=1, keepdims=True))
    for i, piece in enumerate(pieces):
        out_ref[:, :, units + i : units + i + 1] = (
            piece.astype(F32).reshape(n, rows, 1).astype(BF16)
        )


def hidden_kernel(units, parts_ref, *refs):
    out_ref = refs[-1]
    total = jnp.sum(parts_ref[...].astype(F32), axis=0)
    squares = jnp.sum(total[:, units : units + 3], axis=1, keepdims=True)
    factor = scale_of(squares)
    gate, up = factor * total[:, : 2 * PAD], factor * total[:, 2 * PAD :]
    hidden = (gate * jax.nn.sigmoid(gate) * up).astype(BF16)
    for i in range(out_ref.shape[0]):
        out_ref[i] = hidden


def down_kernel(hidden_ref, own_ref, other_ref, out_ref):
    units = own_ref.shape[0]
    hidden = rows_of(hidden_ref).astype(BF16)
    total = dot_nn(hidden[:, :units], own_ref[...])
    total += dot_nn(hidden[:, PAD : PAD + units], other_ref[2 * units : 3 * units])
    out_ref[...] = total.reshape(out_ref.shape).astype(BF16)


def first_kernel(parts_ref, own_ref, first_ref, out_ref):
    branch = jnp.sum(parts_ref[...].astype(F32), axis=0)
    first = (own_ref[...].astype(F32) + 0.5 * branch).astype(BF16)
    first_ref[...] = first
    for i in range(out_ref.shape[0]):
        out_ref[i] = first


def query_kernel(core_ref, rows_ref, gain_ref, q_ref, k_ref, v_ref, other_ref, gates_ref, out_ref):
    n, rows, _ = rows_ref.shape
    dim = q_ref.shape[1]
    stream = rows_of(rows_ref)
    scaled = (stream * gain_ref[...].astype(F32)).astype(BF16)
    is_first = core_ref[0] == 0
    for i, weight in enumerate((q_ref, k_ref, v_ref)):
        own = dot_nn(scaled, weight[...])
        other = dot_nn(scaled, other_ref[:, i * dim : (i + 1) * dim])
        for to, part in enumerate(
            (jnp.where(is_first, own, other), jnp.where(is_first, other, own))
        ):
            out_ref[:, to, :, i * dim : (i + 1) * dim] = part.reshape(n, rows, dim).astype(BF16)
    gates = dot_nt(scaled, gates_ref[...])
    pieces = in_three(jnp.sum(stream * stream, axis=1, keepdims=True))
    for to in range(2):
        columns = [gates[:, to : to + 1], gates[:, 2 + to : 3 + to]]
        columns += [piece.astype(F32) for piece in pieces]
        for i, column in enumerate(columns):
            at = 3 * dim + i
            out_ref[:, to, :, at : at + 1] = column.reshape(n, rows, 1).astype(BF16)


def read_kernel(
    parts_ref,
    state_ref,
    base_ref,
    shift_ref,
    head_gain_ref,
    keys_ref,
    rate_ref,
    correction_ref,
    out_ref,
    recalled,
    queried,
):
    dim = state_ref.shape[2]
    got = jnp.sum(parts_ref[...].astype(F32), axis=0)
    squares = jnp.sum(got[:, 3 * dim + 2 : 3 * dim + 5], axis=1, keepdims=True)
    got = scale_of(squares) * got[:, : 3 * dim + 2]
    queries, keys, values = (got[:, i * dim : (i + 1) * dim] for i in range(3))
    decay_in, blend_in = got[:, 3 * dim : 3 * dim + 1], got[:, 3 * dim + 1 : 3 * dim + 2]

    def unit(v):
        return v * lax.rsqrt(jnp.sum(v * v, axis=1, keepdims=True) + EPS)

    queries, keys = unit(queries) * dim**-0.5, unit(keys)
    inner = decay_in + shift_ref[...]
    soft = jnp.maximum(inner, 0.0) + jnp.log1p(jnp.exp(-jnp.abs(inner)))
    rate = jnp.exp(-jnp.exp(base_ref[...]) * soft)
    beta = jax.nn.sigmoid(blend_in)
    queries_t, keys_t = queries.T, keys.T
    for b in range(state_ref.shape[0]):
        old = state_ref[b]
        recalled[b : b + 1] = jnp.sum(keys_t[:, b : b + 1] * old, axis=0, keepdims=True)
        queried[b : b + 1] = jnp.sum(queries_t[:, b : b + 1] * old, axis=0, keepdims=True)
    correction = beta * (values - rate * recalled[...])
    read = rate * queried[...] + jnp.sum(keys * queries, axis=1, keepdims=True) * correction
    normed = read * lax.rsqrt(jnp.mean(read * read, axis=1, keepdims=True) + EPS)
    normed = (normed * head_gain_ref[...].astype(F32)).astype(BF16)
    for i in range(out_ref.shape[0]):
        out_ref[i] = normed
    keys_ref[...] = keys_t
    rate_ref[...] = rate
    correction_ref[...] = correction


def state_kernel(state_ref, keys_ref, rate_ref, correction_ref, out_ref):
    keys_t, rate, correction = keys_ref[...], rate_ref[...], correction_ref[...]
    for b in range(state_ref.shape[0]):
        new = rate[b : b + 1] * state_ref[b] + keys_t[:, b : b + 1] * correction[b : b + 1]
        out_ref[b] = new


def out_kernel(core_ref, heads_ref, own_ref, other_ref, out_ref):
    n, both, dim = heads_ref.shape
    heads = heads_ref[...].astype(F32)
    zero = heads[:, : both // 2].reshape(n * both // 2, dim).astype(BF16)
    one = heads[:, both // 2 :].reshape(n * both // 2, dim).astype(BF16)
    from_zero, from_one = dot_nn, dot_nn
    is_first = core_ref[0] == 0
    own, other = own_ref[...], other_ref[other_ref.shape[0] - dim :]
    total = from_zero(zero, jnp.where(is_first, own, other))
    total += from_one(one, jnp.where(is_first, other, own))
    out_ref[...] = total.reshape(out_ref.shape).astype(BF16)


def wide_kernel(
    units, parts_ref, first_ref, gain_ref, weights_ref, out_ref, second_ref, held, sems
):
    n, rows, _ = out_ref.shape

    def copy(k):
        return pltpu.make_async_copy(
            weights_ref.at[pl.ds(2 * k, 2), pl.ds(0, 2 * units)], held.at[k], sems.at[k]
        )

    for k in range(AHEAD):
        copy(k).start()
    branch = jnp.sum(parts_ref[...].astype(F32), axis=0)
    second = (first_ref[...].astype(F32) + branch).astype(BF16)
    second_ref[...] = second
    stream = second.astype(F32)
    scaled = (stream * gain_ref[...].astype(F32)).astype(BF16)
    pieces = in_three(jnp.sum(stream * stream, axis=1, keepdims=True))
    for k in range(n):
        for i in range(4):
            out_ref[k, :, i * PAD + units : (i + 1) * PAD] = jnp.zeros((rows, PAD - units), BF16)
        for i, piece in enumerate(pieces):
            out_ref[k, :, units + i : units + i + 1] = piece
    for k in range(n):
        copy(k).wait()
        if k + AHEAD < n:
            copy(k + AHEAD).start()
        for i in range(4):
            weight = held[k, i % 2, (i // 2) * units : (i // 2 + 1) * units]
            out_ref[k, :, i * PAD : i * PAD + units] = dot_nt(scaled, weight).astype(BF16)


def last_kernel(units, hidden_ref, second_ref, weights_ref, out_ref):
    total = jnp.zeros(out_ref.shape, F32)
    for k in range(hidden_ref.shape[0]):
        for i in range(2):
            weight = weights_ref[2 * k + i, 2 * units : 3 * units]
            total += dot_nn(hidden_ref[k, :, i * PAD : i * PAD + units], weight)
    out_ref[...] = (second_ref[...].astype(F32) + 0.5 * total).astype(BF16)


def on_device(
    tokens,
    state,
    gain_pre,
    w_gate_pre,
    w_up_pre,
    w_down_pre,
    gain_mix,
    w_query,
    w_key,
    w_value,
    w_decay,
    w_blend,
    decay_base,
    decay_shift,
    head_gain,
    w_out,
    gain_post,
    w_gate_post,
    w_up_post,
    w_down_post,
):
    n = lax.axis_size(KV)
    rows, width = tokens.shape
    units = w_gate_pre.shape[1]
    seqs, _, dim, _ = state.shape
    core = lax.axis_index("core").reshape(1)
    block = (n, rows, width)
    wide = (n, rows, 4 * PAD)
    narrow = (n, rows, 2 * PAD)

    later = joined(w_gate_post.T, w_up_post.T, w_down_post)
    later = lax.all_gather(later, TP, axis=0, tiled=False)

    gate_t, up_t = w_gate_pre.T, w_up_pre.T
    stream = exchanged(jnp.broadcast_to(tokens[None], block), "z")
    other = from_partner(jnp.concatenate([gate_t, up_t, w_down_pre, w_out], axis=0))
    (sent,) = local_call(
        gate_up_kernel, [(wide, BF16)], (stream, gain_pre[None], gate_t, up_t, other)
    )
    (hidden,) = local_call(
        functools.partial(hidden_kernel, units), [(narrow, BF16)], (exchanged(sent, KV),)
    )
    (sent,) = local_call(
        down_kernel, [(block, BF16)], (exchanged(hidden, KV), w_down_pre, other)
    )
    first, sent = local_call(
        first_kernel, [(tokens.shape, BF16), (block, BF16)], (exchanged(sent, "z"), tokens)
    )

    other_query = from_partner(jnp.concatenate([w_query, w_key, w_value], axis=1))
    pair = 2 * lax.axis_index("z")
    gates = jnp.concatenate(
        [
            lax.dynamic_slice_in_dim(w_decay.T, pair, 2, 0),
            lax.dynamic_slice_in_dim(w_blend.T, pair, 2, 0),
        ],
        axis=0,
    )
    (sent,) = local_call(
        query_kernel,
        [((n, 2, rows, 4 * dim), BF16)],
        (
            core,
            exchanged(sent, "z"),
            gain_mix[None],
            w_query,
            w_key,
            w_value,
            other_query,
            gates,
        ),
        scalars=1,
    )
    got = exchanged(sent.reshape(2 * n, rows, 4 * dim), KVC).reshape(n, 2 * rows, 4 * dim)
    held = state.reshape(seqs, dim, dim)
    keys_t, rate, correction, sent = local_call(
        read_kernel,
        [((dim, seqs), F32), ((seqs, 1), F32), ((seqs, dim), F32), ((n, seqs, dim), BF16)],
        (got, held, decay_base[None], decay_shift[None], head_gain[None]),
        scratch=(pltpu.VMEM((seqs, dim), F32), pltpu.VMEM((seqs, dim), F32)),
    )
    (new_state,) = local_call(
        state_kernel,
        [((seqs, dim, dim), F32)],
        (held, keys_t, rate, correction),
        cost=pl.CostEstimate(flops=1 << 28, bytes_accessed=8 * held.size, transcendentals=0),
    )
    heads = exchanged(sent.reshape(2 * n, rows, dim), KVC).reshape(n, 2 * rows, dim)
    heads, new_state = lax.optimization_barrier((heads, new_state))
    (sent,) = local_call(
        out_kernel, [(block, BF16)], (core, heads, w_out, other), scalars=1
    )

    sent, second = local_call(
        functools.partial(wide_kernel, units),
        [(wide, BF16), (tokens.shape, BF16)],
        (exchanged(sent, "z"), first, gain_post[None], later),
        far=(3,),
        scratch=(pltpu.VMEM((n, 2, 2 * units, width), BF16), pltpu.SemaphoreType.DMA((n,))),
        limit=46 << 20,
    )
    (hidden,) = local_call(
        functools.partial(hidden_kernel, units),
        [(narrow, BF16)],
        (exchanged(sent, KV), *(later,) * 4),
        far=range(1, 5),
        limit=40 << 20,
    )
    (result,) = local_call(
        functools.partial(last_kernel, units),
        [(tokens.shape, BF16)],
        (exchanged(hidden, KV), second, later),
        limit=22 << 20,
    )
    return (result, new_state.reshape(state.shape))


def solution(mesh):
    finer = Mesh(mesh.devices.reshape(4, 4, mesh.shape["tp"] // 2, 2), ALL)
    in_specs = (
        P(TP, KV),
        P(KV, TP, None, None),
        P(KV),
        P(KV, TP),
        P(KV, TP),
        P(TP, KV),
        P(KV),
        P(KV, TP),
        P(KV, TP),
        P(KV, TP),
        P(KV, None),
        P(KV, None),
        P(TP),
        P(TP),
        P(),
        P(TP, KV),
        P(KV),
        P(KV, TP),
        P(KV, TP),
        P(TP, KV),
    )
    out_specs = (P(TP, KV), P(KV, TP, None, None))
    return jax.shard_map(
        on_device, mesh=finer, in_specs=in_specs, out_specs=out_specs, check_vma=False
    )
```
